512 devices in a mesh: sp: 64 (over z, y), tp: 8 (over x, core).
Axes of the slice: x: 4, y: 8, z: 8, core: 2. Of those that a mesh axis runs over, the one named last changes fastest.
Arguments:
- tokens: bfloat16 [16384, 2048], P(('sp', 'tp')), may hold values from -6 to 6
- norm_gain: float32 [2048], replicated, may hold values from 0.1 to 1.9
- w_query: bfloat16 [2048, 1024], P('sp', 'tp'), may hold values from -0.125 to 0.125
- w_forget: bfloat16 [2048, 1024], P('sp', 'tp'), may hold values from -0.125 to 0.125
- w_input: bfloat16 [2048, 1024], P('sp', 'tp'), may hold values from -0.125 to 0.125
- w_outgate: bfloat16 [2048, 1024], P('sp', 'tp'), may hold values from -0.125 to 0.125
- w_bgate: bfloat16 [2048, 1024], P('sp', 'tp'), may hold values from -0.125 to 0.125
- w_cgate: bfloat16 [2048, 1024], P('sp', 'tp'), may hold values from -0.125 to 0.125
- w_value: bfloat16 [2048, 1024], P('sp', 'tp'), may hold values from -0.125 to 0.125
- floor_gap: float32 [8, 128], P('tp'), may hold values from 0 to 0.06
- extra_decay: float32 [16384, 8], P('sp', 'tp'), may hold values from -1 to 0
- start_state: float32 [8, 128, 128], P('tp'), may hold values from -0.02734375 to 0.02734375
- state_gain: float32 [128], replicated, may hold values from 0.1 to 1.9
- conv_taps: float32 [3, 1024], P(None, 'tp'), may hold values from -3 to 3
- out_rec: bfloat16 [1024, 2048], P('tp', 'sp'), may hold values from -0.125 to 0.125
- out_conv: bfloat16 [1024, 2048], P('tp', 'sp'), may hold values from -0.125 to 0.125
Outputs:
- mixed_sum: bfloat16 [16384, 2048], P(('sp', 'tp'))
The draws below stay inside these ranges and needn't reach their ends.
All inputs are finite; a program needn't handle non-finite values.
Results may differ from the reference program's by a relative error of at most 0.018.
Values may be sent and summed in bfloat16 or wider, within the bound.
A program may use at most 64 MiB of HBM per device.

```python
import math
import jax
import jax.numpy as jnp
from jax import lax

D = 2048
HEADS = 8
DK = 128
DV = 128
CONV_CH = 1024
BLOCK = 64
TOK_DEV = 256
TOKENS = 16384
HEAD_GROUPS = 8


def draw_floor_gap(key, part):
    subkeys = jax.random.split(jax.random.fold_in(key, 11), 3)
    share_fast = 0.5
    fast_heads = jax.random.uniform(subkeys[0], (HEADS, 1), jnp.float32) < share_fast
    fast_gap = jnp.exp(jax.random.uniform(subkeys[1], (HEADS, DK), jnp.float32, math.log(0.02), math.log(0.06)))
    slow_gap = jnp.exp(jax.random.uniform(subkeys[2], (HEADS, DK), jnp.float32, math.log(0.1), math.log(0.5))) / TOKENS
    return jnp.where(fast_heads, fast_gap, slow_gap).astype(jnp.float32)


def draw_extra_decay(key, part):
    subkeys = jax.random.split(jax.random.fold_in(key, 23), 3)
    groups = TOKENS // TOK_DEV
    levels = jnp.exp(jax.random.uniform(subkeys[0], (groups, HEADS), jnp.float32, math.log(0.2), math.log(0.8)))
    filtered_signal = -jnp.repeat(levels, TOK_DEV, axis=0) / TOKENS
    location_indices = jax.random.randint(subkeys[1], (2, HEADS), 0, TOKENS)
    stack_tiers = jax.random.uniform(subkeys[2], (2, HEADS), jnp.float32, 0.22, 0.45)
    location_entries = jnp.arange(TOKENS)[None, :, None]
    segment_clusters = jnp.sum(jnp.where(location_entries == location_indices[:, None, :], -stack_tiers[:, None, :], 0.0), axis=0)
    return (filtered_signal + segment_clusters).astype(jnp.float32)


def steps_of(stream_key, extent, cuts, least, high):
    gain = 1.0
    for dim, blocks in cuts:
        steps = jax.random.uniform(jax.random.fold_in(jax.random.fold_in(stream_key, 6), dim), (blocks,), jnp.float32, least / len(cuts), high / len(cuts))
        gain = gain * jnp.repeat(jnp.exp(steps), extent[dim] // blocks).reshape((-1,) + (1,) * (len(extent) - 1 - dim))
    return gain


def bell_draw(own_key, extent, width, bound, cuts=(), dtype=jnp.bfloat16):
    entries = width * jax.random.normal(own_key, extent, jnp.float32)
    if cuts:
        entries = entries * steps_of(own_key, extent, cuts, -0.22, 0.18)
    return jnp.clip(entries, -bound, bound).astype(dtype)


def setup_inputs(seed: int = 0) -> dict:
    arg_keys = jax.random.split(jax.random.key(seed), 17)
    tokens = bell_draw(arg_keys[0], (TOKENS, D), 1.0, 6.0, ((0, 512),))
    norm_gain = jnp.clip(1.0 + 0.18 * jax.random.normal(arg_keys[1], (D,), jnp.float32), 0.1, 1.9)
    w_query = bell_draw(arg_keys[2], (D, HEADS * DK), D ** -0.5, 0.125, ((0, 64), (1, 8)))
    w_forget = bell_draw(arg_keys[3], (D, HEADS * DK), D ** -0.5, 0.125, ((0, 64), (1, 8)))
    w_input = bell_draw(arg_keys[4], (D, HEADS * DV), D ** -0.5, 0.125, ((0, 64), (1, 8)))
    w_outgate = bell_draw(arg_keys[5], (D, HEADS * DV), D ** -0.5, 0.125, ((0, 64), (1, 8)))
    w_bgate = bell_draw(arg_keys[6], (D, CONV_CH), D ** -0.5, 0.125, ((0, 64), (1, 8)))
    w_cgate = bell_draw(arg_keys[7], (D, CONV_CH), D ** -0.5, 0.125, ((0, 64), (1, 8)))
    w_value = bell_draw(arg_keys[8], (D, CONV_CH), D ** -0.5, 0.125, ((0, 64), (1, 8)))
    floor_gap = draw_floor_gap(jax.random.fold_in(arg_keys[16], 71), 0)
    extra_decay = draw_extra_decay(jax.random.fold_in(arg_keys[16], 71), 0)
    start_state = bell_draw(arg_keys[11], (HEADS, DK, DV), (30.0 / TOKENS), 0.02734375, ((0, 8),), jnp.float32)
    state_gain = jnp.clip(1.0 + 0.18 * jax.random.normal(arg_keys[12], (DV,), jnp.float32), 0.1, 1.9)
    conv_taps = bell_draw(arg_keys[13], (3, CONV_CH), 0.6, 3.0, ((1, 8),), jnp.float32)
    out_rec = bell_draw(arg_keys[14], (HEADS * DV, D), (HEADS * DV + CONV_CH) ** -0.5, 0.125, ((0, 8), (1, 64)))
    out_conv = bell_draw(arg_keys[15], (CONV_CH, D), (HEADS * DV + CONV_CH) ** -0.5, 0.125, ((0, 8), (1, 64)))
    return {"tokens": tokens, "norm_gain": norm_gain, "w_query": w_query, "w_forget": w_forget, "w_input": w_input, "w_outgate": w_outgate, "w_bgate": w_bgate, "w_cgate": w_cgate, "w_value": w_value, "floor_gap": floor_gap, "extra_decay": extra_decay, "start_state": start_state, "state_gain": state_gain, "conv_taps": conv_taps, "out_rec": out_rec, "out_conv": out_conv}


eps = 1e-06
highest_precision = lax.Precision.HIGHEST

def rms_scale(values):
    return lax.rsqrt(lax.optimization_barrier(jnp.mean(values * values, axis=-1, keepdims=True)) + eps)

def recurrence(queries, write_in, inputs, log_keep, initial, block_len):
    length, head_count, address_feature_count = queries.shape
    blocks_count = length // block_len

    def blocked(tensor):
        return tensor.reshape(blocks_count, block_len, head_count, tensor.shape[-1]).transpose(0, 2, 1, 3)
    causal = (jnp.arange(block_len)[:, None] >= jnp.arange(block_len)[None, :])[None, :, :, None]

    def advance(memory_state, pieces):
        query_block, write_blk, input_block, keep_blk = pieces
        running_state = jnp.cumsum(keep_blk, axis=1)
        spread = running_state[:, :, None, :] - running_state[:, None, :, :]
        decays = jnp.where(causal, jnp.exp(jnp.minimum(spread, 0.0)), 0.0)
        scores = lax.optimization_barrier(jnp.sum(query_block[:, :, None, :] * write_blk[:, None, :, :] * decays, axis=-1))
        final_output = jnp.einsum('qcp,qpi->qci', query_block * jnp.exp(running_state), memory_state, precision=highest_precision)
        final_output = final_output + jnp.einsum('hts,hsv->htv', scores, input_block, precision=highest_precision)
        final_state = running_state[:, -1, :]
        weighted_value = write_blk * jnp.exp(final_state[:, None, :] - running_state)
        memory_state = memory_state * jnp.exp(final_state)[:, :, None] + jnp.einsum('euz,eul->ezl', weighted_value, input_block, precision=highest_precision)
        return (memory_state, final_output)
    memory_state, output_list = lax.scan(advance, initial, (blocked(queries), blocked(write_in), blocked(inputs), blocked(log_keep)))
    return output_list.transpose(0, 2, 1, 3).reshape(length, head_count, output_list.shape[-1])

def reference(tokens, norm_gain, w_query, w_forget, w_input, w_outgate, w_bgate, w_cgate, w_value, floor_gap, extra_decay, start_state, state_gain, conv_taps, out_rec, out_conv):
    tokens_f = tokens.astype(jnp.float32)
    normed = (tokens_f * rms_scale(tokens_f) * norm_gain).astype(jnp.bfloat16)

    def project(matrix):
        return jnp.dot(normed, matrix, preferred_element_type=jnp.float32).astype(jnp.bfloat16)
    query_raw = project(w_query)
    forget_raw = project(w_forget)
    input_raw = project(w_input)
    outgate_raw = project(w_outgate)
    bgate_raw = project(w_bgate)
    cgate_raw = project(w_cgate)
    value_raw = project(w_value)
    length = normed.shape[0]
    queries = jax.nn.silu(query_raw.astype(jnp.float32)).reshape(length, HEADS, DK)
    write_in = floor_gap[None] * jax.nn.sigmoid(-forget_raw.astype(jnp.float32)).reshape(length, HEADS, DK)
    log_keep = jnp.log1p(-write_in) + extra_decay[:, :, None]
    inputs = input_raw.astype(jnp.float32).reshape(length, HEADS, DV)
    blended_state = recurrence(queries, write_in, inputs, log_keep, start_state, BLOCK)
    gate_out = jax.nn.silu(outgate_raw.astype(jnp.float32)).reshape(length, HEADS, DV)
    rec_out = (blended_state * rms_scale(blended_state) * state_gain * gate_out).reshape(length, HEADS * DV).astype(jnp.bfloat16)
    gated = cgate_raw.astype(jnp.float32) * value_raw.astype(jnp.float32)
    padded = jnp.concatenate([jnp.zeros((2, gated.shape[1]), jnp.float32), gated], axis=0)
    conv_out = conv_taps[0] * padded[:length] + conv_taps[1] * padded[1:length + 1] + conv_taps[2] * padded[2:]
    short_out = (bgate_raw.astype(jnp.float32) * conv_out).astype(jnp.bfloat16)
    rec_width = HEADS * DV // HEAD_GROUPS
    conv_width = CONV_CH // HEAD_GROUPS
    mixed_sum = jnp.zeros((length, out_rec.shape[1]), jnp.float32)
    for group in range(HEAD_GROUPS):
        rec_lo = group * rec_width
        conv_lo = group * conv_width
        partial_value = jnp.dot(rec_out[:, rec_lo:rec_lo + rec_width], out_rec[rec_lo:rec_lo + rec_width], preferred_element_type=jnp.float32)
        partial_value = partial_value + jnp.dot(short_out[:, conv_lo:conv_lo + conv_width], out_conv[conv_lo:conv_lo + conv_width], preferred_element_type=jnp.float32)
        rounded = lax.optimization_barrier(partial_value.astype(jnp.bfloat16))
        mixed_sum = mixed_sum + rounded.astype(jnp.float32)
    return mixed_sum.astype(jnp.bfloat16)
```

```python
import functools

import jax
import jax.numpy as jnp
from jax import lax
from jax.experimental import pallas as pl
from jax.experimental.pallas import tpu as pltpu
from jax.sharding import Mesh
from jax.sharding import PartitionSpec as P

BLOCK = 64
Z, Y, X, C = "sp_0", "sp_1", "tp_0", "tp_1"
SP = (Z, Y)
TP = (X, C)
SP_TP = (Z, Y, X, C)
MESH = pl.DeviceIdType.MESH
EPS = 1e-06
HIGHEST = lax.Precision.HIGHEST
F32 = jnp.float32
BF16 = jnp.bfloat16


def dot(a, b, dims, precision=None):
    return lax.dot_general(a, b, (dims, ((), ())), precision=precision, preferred_element_type=F32)


def silu(v):
    return v * jax.nn.sigmoid(v)


def kernel(
    sizes,
    tokens,
    gain,
    w_query,
    w_forget,
    w_input,
    w_outgate,
    w_bgate,
    w_cgate,
    w_value,
    floor_gap,
    extra_decay,
    start_state,
    state_gain,
    taps,
    out_t,
    out,
    tok,
    wg0,
    wg1,
    wg2,
    wg3,
    wg4,
    normed_ref,
    lk_ref,
    r_ref,
    u_ref,
    w_ref,
    lprev,
    startt,
    ysend,
    yrecv,
    zbuf,
    pref,
    dec,
    back_send,
    back_recv,
    halo_send,
    gext,
    both,
    psend,
    precv,
    ssum,
    xrecv,
    load_sem,
    tokload_sem,
    p1_send,
    p1_recv,
    r_send,
    r_recv,
    tx_send,
    tx_recv,
    td_send,
    td_recv,
    st_send,
    st_recv,
    pd_send,
    pd_recv,
    px_send,
    px_recv,
):
    nz, ny, nx, nc = sizes
    z, y, x, c = (lax.axis_index(name) for name in (Z, Y, X, C))
    groups = (wg0, wg1, wg2, wg3, wg4)
    sources = (
        (w_forget, w_input),
        (w_query, w_outgate),
        (w_cgate, w_value),
        (w_bgate,),
        (out_t,),
    )
    half = tokens.shape[0] // 2
    rows = nx * nc * tokens.shape[0]
    blocks = rows // BLOCK
    dk = floor_gap.shape[1]
    vrows = dk // ny

    tok_load = pltpu.make_async_copy(tokens, tok.at[x, c], tokload_sem)
    tok_load.start()
    for g, parts in enumerate(sources):
        lo = 0
        for part in parts:
            width = part.shape[1]
            for h in range(2):
                pltpu.make_async_copy(
                    part.at[pl.ds(h * half, half)],
                    groups[g].at[z, y, h, :, pl.ds(lo, width)],
                    load_sem.at[g],
                ).start()
            lo += width

    wrap = jnp.where(y == ny - 1, 1, 0)
    unwrap = jnp.where(y == 0, 1, 0)
    after = {Z: lax.rem(z + wrap, nz), Y: lax.rem(y + 1, ny)}
    before = {Z: lax.rem(z + nz - unwrap, nz), Y: lax.rem(y + ny - 1, ny)}
    peers = [{Y: lax.rem(y + d, ny)} for d in range(1, ny)]
    peers += [{Z: lax.rem(z + d, nz)} for d in range(1, nz)]
    peers += [{X: lax.rem(x + d, nx)} for d in range(1, nx)]
    peers += [{C: 1 - c}, after, before]
    barrier = pltpu.get_barrier_semaphore()
    for peer in peers:
        pl.semaphore_signal(barrier, inc=1, device_id=peer, device_id_type=MESH)
    pl.semaphore_wait(barrier, len(peers))

    def remote(src, dst, send, recv, to):
        return pltpu.make_async_remote_copy(
            src_ref=src, dst_ref=dst, send_sem=send, recv_sem=recv, device_id=to, device_id_type=MESH
        )

    pending = []

    def ship(src, dst, send, recv, to):
        copy = remote(src, dst, send, recv, to)
        copy.start()
        pending.append(copy)

    def arrived(ref, send, recv, to):
        remote(ref, ref, send, recv, to).wait_recv()

    nkx = nx // 2

    def tok_ref(direction, k):
        index = lax.rem(x - direction * k + nx, nx)
        if k < nkx:
            return tok.at[index, c]
        lo = 0 if direction > 0 else half
        return tok.at[index, c, pl.ds(lo, half)]

    def tok_ship(direction, k):
        index = lax.rem(x - direction * (k - 1) + nx, nx)
        if k < nkx:
            ref = tok.at[index, c]
        else:
            ref = tok.at[index, c, pl.ds(0 if direction > 0 else half, half)]
        d = 0 if direction > 0 else 1
        to = {X: lax.rem(x + direction + nx, nx)}
        ship(ref, ref, tx_send.at[d, k - 1], tx_recv.at[d, k - 1], to)

    def tok_wait(direction, k):
        d = 0 if direction > 0 else 1
        arrived(
            tok_ref(direction, k),
            tx_send.at[d, k - 1],
            tx_recv.at[d, k - 1],
            {X: lax.rem(x + direction + nx, nx)},
        )

    def tok_across(offset):
        index = lax.rem(x + offset + nx, nx)
        ref = tok.at[index, c]
        at = offset % nx
        ship(ref, ref, td_send.at[at], td_recv.at[at], {C: 1 - c})

    def tok_across_wait(offset):
        index = lax.rem(x + offset + nx, nx)
        ref = tok.at[index, 1 - c]
        at = offset % nx
        arrived(ref, td_send.at[at], td_recv.at[at], {C: 1 - c})

    def first_hop(g):
        w = groups[g]
        for color, (axis, me, n) in enumerate(((Y, y, ny), (Z, z, nz))):
            ref = w.at[z, y, color]
            order = sorted(range(1, n), key=lambda d: -min(d, n - d))
            for d in order:
                remote(
                    ref, ref, p1_send.at[g, color], p1_recv.at[g, color], {axis: lax.rem(me + d, n)}
                ).start()

    def first_ref(g, color):
        w = groups[g]
        if color == 0:
            return w.at[z, pl.ds(0, ny - 1), 0]
        return w.at[pl.ds(0, nz - 1), y, 1]

    def first_wait(g):
        for color, axis in enumerate((Y, Z)):
            ref = first_ref(g, color)
            remote(
                ref, ref, p1_send.at[g, color], p1_recv.at[g, color], {axis: 0}
            ).wait_recv()

    def first_drain(g):
        for color, axis in enumerate((Y, Z)):
            ref = first_ref(g, color)
            remote(
                ref, ref, p1_send.at[g, color], p1_recv.at[g, color], {axis: 0}
            ).wait_send()

    rings = ((Z, z, nz), (Y, y, ny))

    def ring_ref(g, color, direction, k, last):
        axis, me, n = rings[color]
        index = lax.rem(me - direction * k + n, n)
        w = groups[g]
        other = (ny, nz)[color]
        if last:
            part = pl.ds(0 if direction > 0 else other // 2, other // 2)
        else:
            part = pl.ds(0, other)
        if color == 0:
            return w.at[index, part, 0]
        return w.at[part, index, 1]

    def ring_ship(g, k):
        for color in range(2):
            axis, me, n = rings[color]
            if k > n // 2:
                continue
            for d, direction in enumerate((1, -1)):
                ref = ring_ref(g, color, direction, k - 1, k == n // 2)
                ship(
                    ref,
                    ref,
                    r_send.at[g, color, d, k - 1],
                    r_recv.at[g, color, d, k - 1],
                    {axis: lax.rem(me + direction + n, n)},
                )

    def ring_wait(g, k):
        for color in range(2):
            axis, me, n = rings[color]
            if k > n // 2:
                continue
            for d, direction in enumerate((1, -1)):
                ref = ring_ref(g, color, direction, k, k == n // 2)
                arrived(
                    ref,
                    r_send.at[g, color, d, k - 1],
                    r_recv.at[g, color, d, k - 1],
                    {axis: lax.rem(me + direction + n, n)},
                )

    steps = max(nz, ny) // 2

    def front(i):
        for g in range(len(groups)):
            k = i - g + 1
            if k == 1:
                first_wait(g)
                ring_ship(g, 1)
            elif 2 <= k <= steps:
                ring_wait(g, k - 1)
                ring_ship(g, k)
            elif k == steps + 1:
                ring_wait(g, steps)

    def whole(g):
        w = groups[g][...]
        return w.reshape(-1, w.shape[-1])

    def wait_load(g):
        ref = groups[g].at[z, y]
        pltpu.make_async_copy(ref, ref, load_sem.at[g]).wait()

    wait_load(0)
    first_hop(0)
    tok_load.wait()
    for direction in (1, -1):
        tok_ship(direction, 1)
    tok_across(0)
    for g in range(1, len(groups)):
        wait_load(g)
        first_hop(g)
    startt[...] = start_state[0].T.reshape(startt.shape)

    front(0)
    for k in range(1, nkx + 1):
        for direction in (1, -1):
            tok_wait(direction, k)
            if k < nkx:
                tok_ship(direction, k + 1)
                tok_across(-direction * k)
    tok_across(nkx)
    front(1)
    for offset in range(nx):
        tok_across_wait(offset)
    front(2)
    tokens_f = tok[...].reshape(rows, tok.shape[-1]).astype(F32)
    scale = lax.rsqrt(jnp.mean(tokens_f * tokens_f, axis=-1, keepdims=True) + EPS)
    normed_ref[...] = (tokens_f * scale * gain[...]).astype(BF16)

    def project(g):
        raw = dot(normed_ref[...], whole(g), ((1,), (0,)))
        return raw.astype(BF16).astype(F32)

    row = lax.broadcasted_iota(jnp.int32, (BLOCK, BLOCK), 0)
    col = lax.broadcasted_iota(jnp.int32, (BLOCK, BLOCK), 1)
    causal = row >= col
    lower = causal.astype(F32)

    front(3)
    front(4)
    raw = project(0)
    write_in = floor_gap[...] * jax.nn.sigmoid(-raw[:, :dk])
    log_keep = jnp.log1p(-write_in) + extra_decay[...]
    w_ref[...] = write_in
    u_ref[...] = raw[:, dk:]
    memory = None
    total = jnp.zeros((1, dk), F32)
    for b in range(blocks):
        at = pl.ds(b * BLOCK, BLOCK)
        lk = log_keep[b * BLOCK : (b + 1) * BLOCK]
        running = dot(lower, lk, ((1,), (0,)), HIGHEST)
        r_ref[at] = running
        final = running[BLOCK - 1 :]
        lk_ref[pl.ds(b, 1)] = total
        total = total + final
        weighted = w_ref[at] * jnp.exp(final - running)
        fresh = dot(u_ref[at], weighted, ((0,), (0,)), HIGHEST)
        if memory is None:
            lprev[b] = jnp.zeros_like(fresh)
            memory = fresh
        else:
            lprev[b] = memory
            memory = memory * jnp.exp(final) + fresh
    ysend[:, pl.ds(0, vrows)] = memory.reshape(ny, vrows, dk)
    ysend[:, pl.ds(vrows, 8)] = jnp.broadcast_to(total[None], (ny, 8, dk))
    yrecv[y, pl.ds(0, vrows)] = ysend[y, pl.ds(0, vrows)]
    yrecv[y, pl.ds(vrows, 8)] = ysend[y, pl.ds(vrows, 8)]
    front(5)
    for d in range(1, ny):
        to = lax.rem(y + d, ny)
        remote(ysend.at[to], yrecv.at[y], st_send.at[0], st_recv.at[0], {Y: to}).start()

    raw = project(1)
    queries = silu(raw[:, :dk])
    gate_out = silu(raw[:, dk:])
    local, lifted = [], []
    for b in range(blocks):
        at = pl.ds(b * BLOCK, BLOCK)
        running = r_ref[at]
        mid = running[BLOCK // 2 - 1 : BLOCK // 2]
        q = queries[b * BLOCK : (b + 1) * BLOCK]
        scores = dot(
            q * jnp.exp(running - mid), w_ref[at] * jnp.exp(mid - running), ((1,), (1,)), HIGHEST
        )
        scores = jnp.where(causal, scores, 0.0)
        here = dot(scores, u_ref[at], ((1,), (0,)), HIGHEST)
        here = here + dot(q * jnp.exp(running), lprev[b], ((1,), (1,)), HIGHEST)
        local.append(here)
        lifted.append(q * jnp.exp(running + lk_ref[pl.ds(b, 1)]))
    local = jnp.concatenate(local, axis=0)
    lifted = jnp.concatenate(lifted, axis=0)

    front(6)
    ybytes = yrecv.at[pl.ds(0, ny - 1)]
    remote(ybytes, ybytes, st_send.at[0], st_recv.at[0], {Y: 0}).wait()
    so_far = jnp.zeros((vrows, dk), F32)
    logs = jnp.zeros((1, dk), F32)
    for j in range(ny):
        pref[j] = so_far
        dec[pl.ds(j, 1)] = logs
        step = yrecv[j, pl.ds(vrows, 1)]
        so_far = so_far * jnp.exp(step) + yrecv[j, pl.ds(0, vrows)]
        logs = logs + step
    zbuf[z, pl.ds(0, vrows)] = so_far
    zbuf[z, pl.ds(vrows, 8)] = jnp.broadcast_to(logs, (8, dk))

    raw = project(2)
    gated = raw[:, :dk] * raw[:, dk:]
    gext[pl.ds(8, rows)] = gated
    halo_send[...] = gated[rows - 8 :]
    for d in range(1, nz):
        ref = zbuf.at[z]
        remote(ref, ref, st_send.at[1], st_recv.at[1], {Z: lax.rem(z + d, nz)}).start()
    front(7)
    ship(halo_send, gext.at[pl.ds(0, 8)], st_send.at[3], st_recv.at[3], after)
    raw = project(3)
    zbytes = zbuf.at[pl.ds(0, nz - 1)]
    remote(zbytes, zbytes, st_send.at[1], st_recv.at[1], {Z: 0}).wait()
    carry = startt[y]
    for j in range(nz):
        later = carry * jnp.exp(zbuf[j, pl.ds(vrows, 1)]) + zbuf[j, pl.ds(0, vrows)]
        carry = jnp.where(j < z, later, carry)
    for j in range(ny):
        back_send[j] = carry * jnp.exp(dec[pl.ds(j, 1)]) + pref[j]
    back_recv[y] = back_send[y]

    arrived(gext.at[pl.ds(0, 8)], st_send.at[3], st_recv.at[3], after)
    first = jnp.logical_and(z == 0, y == 0)
    halo = jnp.where(first, 0.0, gext[pl.ds(0, 8)])
    gext[pl.ds(0, 8)] = halo
    conv = (
        taps[pl.ds(0, 1)] * gext[pl.ds(6, rows)]
        + taps[pl.ds(1, 1)] * gext[pl.ds(7, rows)]
        + taps[pl.ds(2, 1)] * gext[pl.ds(8, rows)]
    )
    short = (raw * conv).astype(BF16)
    both[:, :, :, pl.ds(dk, dk)] = short.reshape(nx, nc, rows // (nx * nc), dk)
    for d in range(1, ny):
        to = lax.rem(y + d, ny)
        remote(back_send.at[to], back_recv.at[y], st_send.at[2], st_recv.at[2], {Y: to}).start()
    front(8)
    bbytes = back_recv.at[pl.ds(0, ny - 1)]
    remote(bbytes, bbytes, st_send.at[2], st_recv.at[2], {Y: 0}).wait()
    carried = back_recv[...].reshape(dk, dk)
    mixed = local + dot(lifted, carried, ((1,), (1,)), HIGHEST)
    norm = lax.rsqrt(jnp.mean(mixed * mixed, axis=-1, keepdims=True) + EPS)
    rec = (mixed * norm * state_gain[...] * gate_out).astype(BF16)
    both[:, :, :, pl.ds(0, dk)] = rec.reshape(nx, nc, rows // (nx * nc), dk)

    per = rows // (nx * nc)
    weights = whole(4)
    width = out.shape[1]
    chunks = 4
    size = width // chunks
    theirs = both[:, 1 - c].reshape(nx * per, 2 * dk)
    mine = both[:, c].reshape(nx * per, 2 * dk)
    for q in range(chunks):
        at = pl.ds(q * size, size)
        part = dot(theirs, weights[q * size : (q + 1) * size], ((1,), (1,)))
        psend[:, :, at] = part.astype(BF16).reshape(nx, per, size)
        if q > 0:
            last = pl.ds((q - 1) * size, size)
            ship(psend.at[:, :, last], precv.at[:, :, last], pd_send.at[q - 1], pd_recv.at[q - 1], {C: 1 - c})
    own = [dot(mine, weights[q * size : (q + 1) * size], ((1,), (1,))) for q in range(chunks)]
    last = pl.ds((chunks - 1) * size, size)
    ship(psend.at[:, :, last], precv.at[:, :, last], pd_send.at[chunks - 1], pd_recv.at[chunks - 1], {C: 1 - c})

    def push(q):
        at = pl.ds(q * size, size)
        for d in range(1, nx):
            to = lax.rem(x + d, nx)
            ship(ssum.at[to, :, at], xrecv.at[x, :, at], px_send.at[q, d - 1], px_recv.at[q, d - 1], {X: to})

    for q in range(chunks):
        at = pl.ds(q * size, size)
        arrived(precv.at[:, :, at], pd_send.at[q], pd_recv.at[q], {C: 1 - c})
        mix = own[q].reshape(nx, per, size) + precv[:, :, at].astype(F32)
        ssum[:, :, at] = mix.astype(BF16)
        if q > 0:
            push(q - 1)
    push(chunks - 1)
    for q in range(chunks):
        at = pl.ds(q * size, size)
        acc = ssum[x, :, at].astype(F32)
        for d in range(1, nx):
            src = lax.rem(x + nx - d, nx)
            arrived(xrecv.at[src, :, at], px_send.at[q, d - 1], px_recv.at[q, d - 1], {X: src})
            acc = acc + xrecv[src, :, at].astype(F32)
        out[:, at] = acc.astype(BF16)

    for g in range(len(groups)):
        first_drain(g)
    for copy in pending:
        copy.wait_send()


def on_device(sizes, *args):
    (
        tokens,
        norm_gain,
        w_query,
        w_forget,
        w_input,
        w_outgate,
        w_bgate,
        w_cgate,
        w_value,
        floor_gap,
        extra_decay,
        start_state,
        state_gain,
        conv_taps,
        out_rec,
        out_conv,
    ) = args
    nz, ny, nx, nc = sizes
    per, model = tokens.shape
    rows = per * nx * nc
    blocks = rows // BLOCK
    dk = floor_gap.shape[1]
    half = per // 2
    vrows = dk // ny
    out_t = jnp.concatenate([out_rec.T, out_conv.T], axis=1)
    vmem = pl.BlockSpec(memory_space=pltpu.VMEM)
    hbm = pl.BlockSpec(memory_space=pl.ANY)
    dma = pltpu.SemaphoreType.DMA
    steps = max(nz, ny) // 2
    gathered = [(nz, ny, 2, half, k * dk) for k in (2, 2, 2, 1, 2)]
    scratch = [
        pltpu.VMEM((nx, nc, per, model), BF16),
        *[pltpu.VMEM(shape, BF16) for shape in gathered],
        pltpu.VMEM((rows, model), BF16),
        pltpu.VMEM((blocks, dk), F32),
        pltpu.VMEM((rows, dk), F32),
        pltpu.VMEM((rows, dk), F32),
        pltpu.VMEM((rows, dk), F32),
        pltpu.VMEM((blocks, dk, dk), F32),
        pltpu.VMEM((ny, vrows, dk), F32),
        pltpu.VMEM((ny, vrows + 8, dk), F32),
        pltpu.VMEM((ny, vrows + 8, dk), F32),
        pltpu.VMEM((nz, vrows + 8, dk), F32),
        pltpu.VMEM((ny, vrows, dk), F32),
        pltpu.VMEM((ny, dk), F32),
        pltpu.VMEM((ny, vrows, dk), F32),
        pltpu.VMEM((ny, vrows, dk), F32),
        pltpu.VMEM((8, dk), F32),
        pltpu.VMEM((rows + 8, dk), F32),
        pltpu.VMEM((nx, nc, per, 2 * dk), BF16),
        *[pltpu.VMEM((nx, per, model), BF16)] * 4,
        dma((5,)),
        dma,
        dma((5, 2)),
        dma((5, 2)),
        dma((5, 2, 2, steps)),
        dma((5, 2, 2, steps)),
        dma((2, nx // 2)),
        dma((2, nx // 2)),
        dma((nx,)),
        dma((nx,)),
        dma((4,)),
        dma((4,)),
        dma((4,)),
        dma((4,)),
        dma((4, nx - 1)),
        dma((4, nx - 1)),
    ]
    return pl.pallas_call(
        functools.partial(kernel, sizes),
        out_shape=jax.ShapeDtypeStruct((per, model), BF16),
        in_specs=[hbm, vmem] + [hbm] * 7 + [vmem] * 5 + [hbm],
        out_specs=vmem,
        scratch_shapes=scratch,
        compiler_params=pltpu.CompilerParams(collective_id=0, has_side_effects=True),
    )(
        tokens,
        norm_gain[None],
        w_query,
        w_forget,
        w_input,
        w_outgate,
        w_bgate,
        w_cgate,
        w_value,
        floor_gap,
        extra_decay,
        start_state,
        state_gain[None],
        conv_taps,
        out_t,
    )


def on_torus(devices, sizes):
    torus = Mesh(devices.reshape(sizes), SP_TP)
    return jax.shard_map(
        functools.partial(on_device, sizes),
        mesh=torus,
        in_specs=(
            P(SP_TP, None),
            P(),
            P(SP, TP),
            P(SP, TP),
            P(SP, TP),
            P(SP, TP),
            P(SP, TP),
            P(SP, TP),
            P(SP, TP),
            P(TP, None),
            P(SP, TP),
            P(TP, None, None),
            P(),
            P(None, TP),
            P(TP, SP),
            P(TP, SP),
        ),
        out_specs=P(SP_TP, None),
        check_vma=False,
    )


def solution(mesh):
    return on_torus(mesh.devices, (8, 8, 4, 2))
```

```python
import functools

import jax
import jax.numpy as jnp
from jax import lax
from jax.experimental import pallas as pl
from jax.experimental.pallas import tpu as pltpu
from jax.sharding import Mesh
from jax.sharding import PartitionSpec as P

BLOCK = 64
Z, Y, X, C = "sp_0", "sp_1", "tp_0", "tp_1"
SP = (Z, Y)
TP = (X, C)
SP_TP = (Z, Y, X, C)
MESH = pl.DeviceIdType.MESH
EPS = 1e-06
HIGHEST = lax.Precision.HIGHEST
F32 = jnp.float32
BF16 = jnp.bfloat16


def dot(a, b, dims, precision=None):
    return lax.dot_general(a, b, (dims, ((), ())), precision=precision, preferred_element_type=F32)


def silu(v):
    return v * jax.nn.sigmoid(v)


def kernel(
    sizes,
    tokens,
    gain,
    w_query,
    w_forget,
    w_input,
    w_outgate,
    w_bgate,
    w_cgate,
    w_value,
    floor_gap,
    extra_decay,
    start_state,
    state_gain,
    taps,
    rec_t,
    conv_t,
    out,
    tok,
    wg0,
    wg1,
    wg2,
    wg3,
    wg4,
    wg5,
    normed_ref,
    off_ref,
    r_ref,
    u_ref,
    w_ref,
    lprev,
    startt,
    ysend,
    yrecv,
    zbuf,
    pref,
    dec,
    back_send,
    back_recv,
    halo_send,
    gext,
    both,
    psend,
    precv,
    ssum,
    xrecv,
    gain_v,
    gap_v,
    extra_v,
    start_v,
    sgain_v,
    taps_v,
    load_sem,
    p1_send,
    p1_recv,
    p1r_recv,
    r_send,
    r_recv,
    tx_send,
    tx_recv,
    td_send,
    td_recv,
    st_send,
    st_recv,
    pd_send,
    pd_recv,
    px_send,
    px_recv,
):
    nz, ny, nx, nc = sizes
    n = nz
    z, y, x, c = (lax.axis_index(name) for name in (Z, Y, X, C))
    groups = (wg0, wg1, wg2, wg3, wg4, wg5)
    sources = (
        (w_forget,),
        (w_input,),
        (w_query, w_outgate),
        (w_cgate, w_value),
        (w_bgate,),
        (rec_t, conv_t),
    )
    direct, relayed = (0, 1, 2), (3, 4, 5)
    half = tokens.shape[0] // 2
    rows = nx * nc * tokens.shape[0]
    blocks = rows // BLOCK
    dk = floor_gap.shape[1]
    vrows = dk // ny

    wrap = jnp.where(y == ny - 1, 1, 0)
    unwrap = jnp.where(y == 0, 1, 0)
    after = {Z: lax.rem(z + wrap, nz), Y: lax.rem(y + 1, ny)}
    before = {Z: lax.rem(z + nz - unwrap, nz), Y: lax.rem(y + ny - 1, ny)}
    far_first = sorted(range(1, n), key=lambda d: -min(d, n - d))
    peers = [{Y: lax.rem(y + d, ny)} for d in far_first]
    peers += [{Z: lax.rem(z + d, nz)} for d in far_first]
    peers += [{X: lax.rem(x + d, nx)} for d in range(1, nx)]
    peers += [{C: 1 - c}, after, before]
    barrier = pltpu.get_barrier_semaphore()
    for peer in peers:
        pl.semaphore_signal(barrier, inc=1, device_id=peer, device_id_type=MESH)

    tok_load = pltpu.make_async_copy(tokens, tok.at[x, c], load_sem.at[6])

    def load(g):
        lo = 0
        for part in sources[g]:
            width = part.shape[1]
            for h in range(2):
                pltpu.make_async_copy(
                    part.at[pl.ds(h * half, half)],
                    groups[g].at[z, y, h, :, pl.ds(lo, width)],
                    load_sem.at[g],
                ).start()
            lo += width

    def wait_load(g):
        ref = groups[g].at[z, y]
        pltpu.make_async_copy(ref, ref, load_sem.at[g]).wait()

    load(0)
    load(1)
    tok_load.start()
    for g in range(2, 6):
        load(g)
    small = [
        pltpu.make_async_copy(src, dst, load_sem.at[7 + i])
        for i, (src, dst) in enumerate(
            (
                (gain, gain_v),
                (floor_gap, gap_v),
                (extra_decay, extra_v),
                (start_state, start_v),
                (state_gain, sgain_v),
                (taps, taps_v),
            )
        )
    ]
    for copy in small:
        copy.start()
    for g in range(6):
        wait_load(g)
    tok_load.wait()
    pl.semaphore_wait(barrier, len(peers))

    def remote(src, dst, send, recv, to):
        return pltpu.make_async_remote_copy(
            src_ref=src, dst_ref=dst, send_sem=send, recv_sem=recv, device_id=to, device_id_type=MESH
        )

    pending = []

    def ship(src, dst, send, recv, to):
        copy = remote(src, dst, send, recv, to)
        copy.start()
        pending.append(copy)

    def landed(ref, recv):
        remote(ref, ref, recv, recv, {C: 1 - c}).wait_recv()

    def left(ref, send):
        remote(ref, ref, send, send, {C: 1 - c}).wait_send()

    nkx = nx // 2

    def tok_part(index, direction, k):
        if k < nkx:
            return tok.at[index, c]
        return tok.at[index, c, pl.ds(0 if direction > 0 else half, half)]

    def tok_ship(direction, k):
        ref = tok_part(lax.rem(x - direction * (k - 1) + nx, nx), direction, k)
        d = 0 if direction > 0 else 1
        to = {X: lax.rem(x + direction + nx, nx)}
        ship(ref, ref, tx_send.at[d, k - 1], tx_recv.at[d, k - 1], to)

    def tok_wait(direction, k):
        d = 0 if direction > 0 else 1
        landed(tok_part(lax.rem(x - direction * k + nx, nx), direction, k), tx_recv.at[d, k - 1])

    def tok_across(offset):
        ref = tok.at[lax.rem(x + offset + nx, nx), c]
        ship(ref, ref, td_send.at[offset % nx], td_recv.at[offset % nx], {C: 1 - c})

    def tok_across_wait(offset):
        landed(tok.at[lax.rem(x + offset + nx, nx), 1 - c], td_recv.at[offset % nx])

    lines = ((Y, y), (Z, z))

    def first_hop(g):
        for color, (axis, me) in enumerate(lines):
            ref = groups[g].at[z, y, color]
            for d in far_first:
                remote(
                    ref, ref, p1_send.at[g], p1_recv.at[g], {axis: lax.rem(me + d, n)}
                ).start()

    def first_wait(g):
        landed(groups[g].at[pl.ds(0, n - 1), 0], p1_recv.at[g])

    def relay_parts(k, direction):
        if k < n // 2:
            return relayed
        return relayed[:1] if direction > 0 else relayed[1:]

    def relay_ship(k):
        for color, (axis, me) in enumerate(lines):
            for direction in (1, -1):
                index = lax.rem(me - direction * (k - 1) + n, n)
                for g in relay_parts(k, direction):
                    w = groups[g]
                    ref = w.at[z, index, 0] if color == 0 else w.at[index, y, 1]
                    to = {axis: lax.rem(me + direction + n, n)}
                    remote(ref, ref, p1_send.at[g], p1r_recv.at[k - 1, g - 3], to).start()

    def relay_wait(k):
        for g in relayed:
            landed(groups[g].at[pl.ds(0, 2 if k < n // 2 else 1), 0], p1r_recv.at[k - 1, g - 3])

    rings = ((Z, z), (Y, y))
    steps = n // 2

    def ring_ship(g, k):
        w = groups[g]
        for color, (axis, me) in enumerate(rings):
            for direction in (1, -1):
                index = lax.rem(me - direction * (k - 1) + n, n)
                if k == steps:
                    part = pl.ds(0 if direction > 0 else n // 2, n // 2)
                else:
                    part = pl.ds(0, n)
                ref = w.at[index, part, 0] if color == 0 else w.at[part, index, 1]
                to = {axis: lax.rem(me + direction + n, n)}
                remote(ref, ref, r_send.at[g], r_recv.at[g, k - 1], to).start()

    def ring_wait(g, k):
        landed(groups[g].at[pl.ds(0, 2 if k < steps else 1)], r_recv.at[g, k - 1])

    sent, seen = [0] * 6, [0] * 6
    relayed_to = [0, 0]

    def see(g, k):
        while seen[g] < k:
            seen[g] += 1
            ring_wait(g, seen[g])

    def pass_on(k, *which):
        for g in which:
            while sent[g] < min(k, steps):
                see(g, sent[g])
                sent[g] += 1
                ring_ship(g, sent[g])

    def done(g):
        pass_on(steps, g)
        see(g, steps)

    def relay_on(k):
        while relayed_to[0] < min(k, steps):
            while relayed_to[1] < relayed_to[0]:
                relayed_to[1] += 1
                relay_wait(relayed_to[1])
            relayed_to[0] += 1
            relay_ship(relayed_to[0])

    def relay_done():
        relay_on(steps)
        relay_wait(steps)

    def whole(g):
        w = groups[g][...]
        return w.reshape(-1, w.shape[-1])

    def project(g):
        raw = dot(normed_ref[...], whole(g), ((1,), (0,)))
        return raw.astype(BF16).astype(F32)

    for g in direct[:2]:
        first_hop(g)
    for direction in (1, -1):
        tok_ship(direction, 1)
    tok_across(0)
    first_hop(2)
    relay_on(1)
    for copy in small:
        copy.wait()
    startt[...] = start_v[0].T.reshape(startt.shape)

    first_wait(0)
    pass_on(1, 0)
    first_wait(1)
    pass_on(1, 1)
    relay_on(2)
    for k in range(1, nkx):
        for direction in (1, -1):
            tok_wait(direction, k)
            tok_ship(direction, k + 1)
            tok_across(-direction * k)
    pass_on(2, 0, 1)
    first_wait(2)
    pass_on(1, 2)
    relay_on(3)
    for direction in (1, -1):
        tok_wait(direction, nkx)
    tok_across(nkx)
    pass_on(3, 0, 1)
    pass_on(2, 2)
    relay_on(4)
    for offset in range(nx):
        tok_across_wait(offset)
    tokens_f = tok[...].reshape(rows, tok.shape[-1]).astype(F32)
    scale = lax.rsqrt(jnp.mean(tokens_f * tokens_f, axis=-1, keepdims=True) + EPS)
    normed_ref[...] = (tokens_f * scale * gain_v[...]).astype(BF16)
    pass_on(4, 0, 1)
    relay_done()
    pass_on(1, 3)

    row = lax.broadcasted_iota(jnp.int32, (BLOCK, BLOCK), 0)
    col = lax.broadcasted_iota(jnp.int32, (BLOCK, BLOCK), 1)
    causal = row >= col
    lower = causal.astype(F32)

    done(0)
    raw = project(0)
    write_in = gap_v[...] * jax.nn.sigmoid(-raw)
    log_keep = jnp.log1p(-write_in)
    w_ref[...] = write_in
    done(1)
    u_ref[...] = project(1)
    memory = None
    total = jnp.zeros((1, dk), F32)
    for b in range(blocks):
        at = pl.ds(b * BLOCK, BLOCK)
        lk = log_keep[b * BLOCK : (b + 1) * BLOCK]
        extra = jnp.where(causal, extra_v[:, at], 0.0)
        running = dot(lower, lk, ((1,), (0,)), HIGHEST) + jnp.sum(extra, axis=1, keepdims=True)
        r_ref[at] = running
        final = running[BLOCK - 1 :]
        off_ref[pl.ds(b, 1)] = total
        total = total + final
        weighted = w_ref[at] * jnp.exp(final - running)
        fresh = dot(u_ref[at], weighted, ((0,), (0,)), HIGHEST)
        if memory is None:
            lprev[b] = jnp.zeros_like(fresh)
            memory = fresh
        else:
            lprev[b] = memory
            memory = memory * jnp.exp(final) + fresh
    ysend[:, pl.ds(0, vrows)] = memory.reshape(ny, vrows, dk)
    ysend[:, pl.ds(vrows, 8)] = jnp.broadcast_to(total[None], (ny, 8, dk))
    yrecv[y] = ysend[y]
    for d in far_first:
        to = lax.rem(y + d, ny)
        remote(ysend.at[to], yrecv.at[y], st_send.at[0], st_recv.at[0], {Y: to}).start()
    pass_on(1, 4, 5)
    pass_on(3, 2)
    pass_on(2, 3, 4, 5)
    pass_on(4, 2)

    done(2)
    raw = project(2)
    queries = silu(raw[:, :dk])
    gate_out = silu(raw[:, dk:])
    landed(yrecv.at[pl.ds(0, ny - 1)], st_recv.at[0])
    so_far = jnp.zeros((vrows, dk), F32)
    logs = jnp.zeros((1, dk), F32)
    for j in range(ny):
        pref[j] = so_far
        dec[pl.ds(j, 1)] = logs
        step = yrecv[j, pl.ds(vrows, 1)]
        so_far = so_far * jnp.exp(step) + yrecv[j, pl.ds(0, vrows)]
        logs = logs + step
    zbuf[z, pl.ds(0, vrows)] = so_far
    zbuf[z, pl.ds(vrows, 8)] = jnp.broadcast_to(logs, (8, dk))
    for d in far_first:
        ref = zbuf.at[z]
        remote(ref, ref, st_send.at[1], st_recv.at[1], {Z: lax.rem(z + d, nz)}).start()
    pass_on(3, 3, 4, 5)

    local, lifted = [], []
    for b in range(blocks):
        at = pl.ds(b * BLOCK, BLOCK)
        running = r_ref[at]
        mid = running[BLOCK // 2 - 1 : BLOCK // 2]
        q = queries[b * BLOCK : (b + 1) * BLOCK]
        scores = dot(
            q * jnp.exp(running - mid), w_ref[at] * jnp.exp(mid - running), ((1,), (1,)), HIGHEST
        )
        scores = jnp.where(causal, scores, 0.0)
        here = dot(scores, u_ref[at], ((1,), (0,)), HIGHEST)
        here = here + dot(q * jnp.exp(running), lprev[b], ((1,), (1,)), HIGHEST)
        local.append(here)
        lifted.append(q * jnp.exp(running + off_ref[pl.ds(b, 1)]))
    local = jnp.concatenate(local, axis=0)
    lifted = jnp.concatenate(lifted, axis=0)

    landed(zbuf.at[pl.ds(0, nz - 1)], st_recv.at[1])
    carry = startt[y]
    for j in range(nz):
        later = carry * jnp.exp(zbuf[j, pl.ds(vrows, 1)]) + zbuf[j, pl.ds(0, vrows)]
        carry = jnp.where(j < z, later, carry)
    for j in range(ny):
        back_send[j] = carry * jnp.exp(dec[pl.ds(j, 1)]) + pref[j]
    back_recv[y] = back_send[y]
    for d in far_first:
        to = lax.rem(y + d, ny)
        remote(back_send.at[to], back_recv.at[y], st_send.at[2], st_recv.at[2], {Y: to}).start()
    pass_on(4, 3, 4, 5)

    per = rows // (nx * nc)
    done(3)
    raw = project(3)
    gated = raw[:, :dk] * raw[:, dk:]
    gext[pl.ds(8, rows)] = gated
    halo_send[...] = gated[rows - 8 :]
    done(4)
    outer = project(4)
    ship(halo_send, gext.at[pl.ds(0, 8)], st_send.at[3], st_recv.at[3], after)
    landed(gext.at[pl.ds(0, 8)], st_recv.at[3])
    first = jnp.logical_and(z == 0, y == 0)
    halo = jnp.where(first, 0.0, gext[pl.ds(0, 8)])
    gext[pl.ds(0, 8)] = halo
    conv = (
        taps_v[pl.ds(0, 1)] * gext[pl.ds(6, rows)]
        + taps_v[pl.ds(1, 1)] * gext[pl.ds(7, rows)]
        + taps_v[pl.ds(2, 1)] * gext[pl.ds(8, rows)]
    )
    short = (outer * conv).astype(BF16)
    both[:, :, :, pl.ds(dk, dk)] = short.reshape(nx, nc, per, dk)

    landed(back_recv.at[pl.ds(0, ny - 1)], st_recv.at[2])
    carried = back_recv[...].reshape(dk, dk)
    mixed = local + dot(lifted, carried, ((1,), (1,)), HIGHEST)
    norm = lax.rsqrt(jnp.mean(mixed * mixed, axis=-1, keepdims=True) + EPS)
    rec = (mixed * norm * sgain_v[...] * gate_out).astype(BF16)
    both[:, :, :, pl.ds(0, dk)] = rec.reshape(nx, nc, per, dk)
    done(5)

    weights = whole(5)
    width = out.shape[1]
    chunks = 4
    size = width // chunks
    theirs = both[:, 1 - c].reshape(nx * per, 2 * dk)
    mine = both[:, c].reshape(nx * per, 2 * dk)

    def pair_ship(q):
        at = pl.ds(q * size, size)
        ship(psend.at[:, :, at], precv.at[:, :, at], pd_send.at[q], pd_recv.at[q], {C: 1 - c})

    own = []
    for q in range(chunks):
        part = dot(theirs, weights[q * size : (q + 1) * size], ((1,), (1,)))
        psend[:, :, pl.ds(q * size, size)] = part.astype(BF16).reshape(nx, per, size)
        own.append(dot(mine, weights[q * size : (q + 1) * size], ((1,), (1,))))
        pair_ship(q)

    def push(q):
        at = pl.ds(q * size, size)
        for d in range(1, nx):
            to = lax.rem(x + d, nx)
            ship(ssum.at[to, :, at], xrecv.at[x, :, at], px_send.at[q, d - 1], px_recv.at[q, d - 1], {X: to})

    for q in range(chunks):
        at = pl.ds(q * size, size)
        landed(precv.at[:, :, at], pd_recv.at[q])
        mix = own[q].reshape(nx, per, size) + precv[:, :, at].astype(F32)
        ssum[:, :, at] = mix.astype(BF16)
        if q > 0:
            push(q - 1)
    push(chunks - 1)
    for q in range(chunks):
        at = pl.ds(q * size, size)
        acc = ssum[x, :, at].astype(F32)
        for d in range(1, nx):
            src = lax.rem(x + nx - d, nx)
            landed(xrecv.at[src, :, at], px_recv.at[q, d - 1])
            acc = acc + xrecv[src, :, at].astype(F32)
        out[:, at] = acc.astype(BF16)

    for g in range(6):
        left(groups[g].at[pl.ds(0, n - 1), 0], p1_send.at[g])
        left(groups[g].at[pl.ds(0, n - 1)], r_send.at[g])
    left(ysend.at[pl.ds(0, ny - 1)], st_send.at[0])
    left(zbuf.at[pl.ds(0, nz - 1)], st_send.at[1])
    left(back_send.at[pl.ds(0, ny - 1)], st_send.at[2])
    for copy in pending:
        copy.wait_send()


def on_device(sizes, *args):
    (
        tokens,
        norm_gain,
        w_query,
        w_forget,
        w_input,
        w_outgate,
        w_bgate,
        w_cgate,
        w_value,
        floor_gap,
        extra_decay,
        start_state,
        state_gain,
        conv_taps,
        out_rec,
        out_conv,
    ) = args
    nz, ny, nx, nc = sizes
    per, model = tokens.shape
    rows = per * nx * nc
    blocks = rows // BLOCK
    dk = floor_gap.shape[1]
    half = per // 2
    vrows = dk // ny
    vmem = pl.BlockSpec(memory_space=pltpu.VMEM)
    hbm = pl.BlockSpec(memory_space=pl.ANY)
    dma = pltpu.SemaphoreType.DMA
    steps = nz // 2
    gathered = [(nz, ny, 2, half, k * dk) for k in (1, 1, 2, 2, 1, 2)]
    operands = (
        tokens,
        norm_gain[None],
        w_query,
        w_forget,
        w_input,
        w_outgate,
        w_bgate,
        w_cgate,
        w_value,
        floor_gap,
        extra_decay.T,
        start_state,
        state_gain[None],
        conv_taps,
        out_rec.T,
        out_conv.T,
    )
    small = (1, 9, 10, 11, 12, 13)
    scratch = [
        pltpu.VMEM((nx, nc, per, model), BF16),
        *[pltpu.VMEM(shape, BF16) for shape in gathered],
        pltpu.VMEM((rows, model), BF16),
        pltpu.VMEM((blocks, dk), F32),
        pltpu.VMEM((rows, dk), F32),
        pltpu.VMEM((rows, dk), F32),
        pltpu.VMEM((rows, dk), F32),
        pltpu.VMEM((blocks, dk, dk), F32),
        pltpu.VMEM((ny, vrows, dk), F32),
        pltpu.VMEM((ny, vrows + 8, dk), F32),
        pltpu.VMEM((ny, vrows + 8, dk), F32),
        pltpu.VMEM((nz, vrows + 8, dk), F32),
        pltpu.VMEM((ny, vrows, dk), F32),
        pltpu.VMEM((ny, dk), F32),
        pltpu.VMEM((ny, vrows, dk), F32),
        pltpu.VMEM((ny, vrows, dk), F32),
        pltpu.VMEM((8, dk), F32),
        pltpu.VMEM((rows + 8, dk), F32),
        pltpu.VMEM((nx, nc, per, 2 * dk), BF16),
        *[pltpu.VMEM((nx, per, model), BF16)] * 4,
        *[pltpu.VMEM(operands[i].shape, F32) for i in small],
        dma((13,)),
        dma((6,)),
        dma((3,)),
        dma((steps, 3)),
        dma((6,)),
        dma((6, steps)),
        dma((2, nx // 2)),
        dma((2, nx // 2)),
        dma((nx,)),
        dma((nx,)),
        dma((4,)),
        dma((4,)),
        dma((4,)),
        dma((4,)),
        dma((4, nx - 1)),
        dma((4, nx - 1)),
    ]
    return pl.pallas_call(
        functools.partial(kernel, sizes),
        out_shape=jax.ShapeDtypeStruct((per, model), BF16),
        in_specs=[hbm] * len(operands),
        out_specs=vmem,
        scratch_shapes=scratch,
        compiler_params=pltpu.CompilerParams(collective_id=0, has_side_effects=True),
    )(*operands)


def on_torus(devices, sizes):
    torus = Mesh(devices.reshape(sizes), SP_TP)
    return jax.shard_map(
        functools.partial(on_device, sizes),
        mesh=torus,
        in_specs=(
            P(SP_TP, None),
            P(),
            P(SP, TP),
            P(SP, TP),
            P(SP, TP),
            P(SP, TP),
            P(SP, TP),
            P(SP, TP),
            P(SP, TP),
            P(TP, None),
            P(SP, TP),
            P(TP, None, None),
            P(),
            P(None, TP),
            P(TP, SP),
            P(TP, SP),
        ),
        out_specs=P(SP_TP, None),
        check_vma=False,
    )


def solution(mesh):
    return on_torus(mesh.devices, (8, 8, 4, 2))
```

```python
import functools

import jax
import jax.numpy as jnp
from jax import lax
from jax.experimental import pallas as pl
from jax.experimental.pallas import tpu as pltpu
from jax.sharding import Mesh
from jax.sharding import PartitionSpec as P

BLOCK = 64
Z, Y, X, C = "sp_0", "sp_1", "tp_0", "tp_1"
SP = (Z, Y)
TP = (X, C)
SP_TP = (Z, Y, X, C)
MESH = pl.DeviceIdType.MESH
EPS = 1e-06
HIGHEST = lax.Precision.HIGHEST
F32 = jnp.float32
BF16 = jnp.bfloat16


def dot(a, b, dims, precision=None):
    return lax.dot_general(a, b, (dims, ((), ())), precision=precision, preferred_element_type=F32)


def silu(v):
    return v * jax.nn.sigmoid(v)


def kernel(
    sizes,
    tokens,
    gain,
    w_query,
    w_forget,
    w_input,
    w_outgate,
    w_bgate,
    w_cgate,
    w_value,
    floor_gap,
    extra_decay,
    start_state,
    state_gain,
    taps,
    rec_t,
    conv_t,
    out,
    tok,
    wg0,
    wg1,
    wg2,
    wg3,
    wg4,
    wg5,
    normed_ref,
    off_ref,
    r_ref,
    u_ref,
    w_ref,
    lprev,
    startt,
    ysend,
    yrecv,
    zbuf,
    pref,
    dec,
    back_send,
    back_recv,
    halo_send,
    gext,
    both,
    psend,
    precv,
    ssum,
    xrelay,
    xrecv,
    gain_v,
    gap_v,
    extra_v,
    start_v,
    sgain_v,
    taps_v,
    load_sem,
    p1_send,
    p1_recv,
    p1r_recv,
    r_send,
    r_recv,
    tx_send,
    tx_recv,
    td_send,
    td_recv,
    st_send,
    st_recv,
    pd_send,
    pd_recv,
    px_send,
    px_recv,
):
    nz, ny, nx, nc = sizes
    n = nz
    z, y, x, c = (lax.axis_index(name) for name in (Z, Y, X, C))
    groups = (wg0, wg1, wg2, wg3, wg4, wg5)
    sources = (
        (w_forget,),
        (w_input,),
        (w_query, w_outgate),
        (w_cgate, w_value),
        (w_bgate,),
        (rec_t, conv_t),
    )
    half = tokens.shape[0] // 2
    rows = nx * nc * tokens.shape[0]
    blocks = rows // BLOCK
    dk = floor_gap.shape[1]
    vrows = dk // ny

    wrap = jnp.where(y == ny - 1, 1, 0)
    unwrap = jnp.where(y == 0, 1, 0)
    after = {Z: lax.rem(z + wrap, nz), Y: lax.rem(y + 1, ny)}
    before = {Z: lax.rem(z + nz - unwrap, nz), Y: lax.rem(y + ny - 1, ny)}
    far_first = sorted(range(1, n), key=lambda d: -min(d, n - d))
    peers = [{Y: lax.rem(y + d, ny)} for d in far_first]
    peers += [{Z: lax.rem(z + d, nz)} for d in far_first]
    peers += [{X: lax.rem(x + d, nx)} for d in range(1, nx)]
    peers += [{C: 1 - c}, after, before]
    barrier = pltpu.get_barrier_semaphore()
    for peer in peers:
        pl.semaphore_signal(barrier, inc=1, device_id=peer, device_id_type=MESH)

    tok_load = pltpu.make_async_copy(tokens, tok.at[x, c], load_sem.at[6])

    def load(g):
        lo = 0
        for part in sources[g]:
            width = part.shape[1]
            for h in range(2):
                pltpu.make_async_copy(
                    part.at[pl.ds(h * half, half)],
                    groups[g].at[z, y, h, :, pl.ds(lo, width)],
                    load_sem.at[g],
                ).start()
            lo += width

    def wait_load(g):
        ref = groups[g].at[z, y]
        pltpu.make_async_copy(ref, ref, load_sem.at[g]).wait()

    load(0)
    load(1)
    tok_load.start()
    for g in range(2, 6):
        load(g)
    small = [
        pltpu.make_async_copy(src, dst, load_sem.at[7 + i])
        for i, (src, dst) in enumerate(
            (
                (gain, gain_v),
                (floor_gap, gap_v),
                (extra_decay, extra_v),
                (start_state, start_v),
                (state_gain, sgain_v),
                (taps, taps_v),
            )
        )
    ]
    for copy in small:
        copy.start()
    for g in range(6):
        wait_load(g)
    tok_load.wait()
    pl.semaphore_wait(barrier, len(peers))

    def remote(src, dst, send, recv, to):
        return pltpu.make_async_remote_copy(
            src_ref=src, dst_ref=dst, send_sem=send, recv_sem=recv, device_id=to, device_id_type=MESH
        )

    pending = []

    def ship(src, dst, send, recv, to):
        copy = remote(src, dst, send, recv, to)
        copy.start()
        pending.append(copy)

    def landed(ref, recv):
        remote(ref, ref, recv, recv, {C: 1 - c}).wait_recv()

    def left(ref, send):
        remote(ref, ref, send, send, {C: 1 - c}).wait_send()

    nkx = nx // 2

    def tok_part(index, direction, k):
        if k < nkx:
            return tok.at[index, c]
        return tok.at[index, c, pl.ds(0 if direction > 0 else half, half)]

    def tok_ship(direction, k):
        ref = tok_part(lax.rem(x - direction * (k - 1) + nx, nx), direction, k)
        d = 0 if direction > 0 else 1
        to = {X: lax.rem(x + direction + nx, nx)}
        ship(ref, ref, tx_send.at[d, k - 1], tx_recv.at[d, k - 1], to)

    def tok_wait(direction, k):
        d = 0 if direction > 0 else 1
        landed(tok_part(lax.rem(x - direction * k + nx, nx), direction, k), tx_recv.at[d, k - 1])

    def tok_across(offset):
        ref = tok.at[lax.rem(x + offset + nx, nx), c]
        ship(ref, ref, td_send.at[offset % nx], td_recv.at[offset % nx], {C: 1 - c})

    def tok_across_wait(offset):
        landed(tok.at[lax.rem(x + offset + nx, nx), 1 - c], td_recv.at[offset % nx])

    lines = ((Y, y), (Z, z))

    def first_hop(g):
        for color, (axis, me) in enumerate(lines):
            ref = groups[g].at[z, y, color]
            for d in far_first:
                remote(
                    ref, ref, p1_send.at[g], p1_recv.at[g], {axis: lax.rem(me + d, n)}
                ).start()

    def first_wait(g):
        landed(groups[g].at[pl.ds(0, n - 1), 0], p1_recv.at[g])

    relayed = (4, 5)
    steps = n // 2

    def relay_ship(k):
        for color, (axis, me) in enumerate(lines):
            for direction in (1, -1):
                index = lax.rem(me - direction * (k - 1) + n, n)
                to = {axis: lax.rem(me + direction + n, n)}
                for g in relayed:
                    if k == steps and (g == 4) == (direction > 0):
                        continue
                    w = groups[g]
                    ref = w.at[z, index, 0] if color == 0 else w.at[index, y, 1]
                    remote(ref, ref, p1_send.at[g], p1r_recv.at[k - 1, g - 4], to).start()

    def relay_wait(k):
        for g in relayed:
            landed(groups[g].at[pl.ds(0, 2 if k < steps else 1), 0], p1r_recv.at[k - 1, g - 4])

    relay = [0, 0]

    def relay_seen(k):
        while relay[1] < k:
            relay[1] += 1
            relay_wait(relay[1])

    def relay_on(k):
        while relay[0] < min(k, steps):
            relay_seen(relay[0])
            relay[0] += 1
            relay_ship(relay[0])

    def relay_done():
        relay_on(steps)
        relay_seen(steps)

    rings = ((Z, z), (Y, y))

    def ring_ship(g, k):
        w = groups[g]
        for color, (axis, me) in enumerate(rings):
            for direction in (1, -1):
                index = lax.rem(me - direction * (k - 1) + n, n)
                if k == steps:
                    part = pl.ds(0 if direction > 0 else n // 2, n // 2)
                else:
                    part = pl.ds(0, n)
                ref = w.at[index, part, 0] if color == 0 else w.at[part, index, 1]
                to = {axis: lax.rem(me + direction + n, n)}
                remote(ref, ref, r_send.at[g], r_recv.at[g, k - 1], to).start()

    def ring_wait(g, k):
        landed(groups[g].at[pl.ds(0, 2 if k < steps else 1)], r_recv.at[g, k - 1])

    sent, seen = [0] * 6, [0] * 6

    def see(g, k):
        while seen[g] < k:
            seen[g] += 1
            ring_wait(g, seen[g])

    def pass_on(k, *which):
        for g in which:
            while sent[g] < min(k, steps):
                see(g, sent[g])
                sent[g] += 1
                ring_ship(g, sent[g])

    def done(g):
        pass_on(steps, g)
        see(g, steps)

    def whole(g):
        w = groups[g][...]
        return w.reshape(-1, w.shape[-1])

    def project(g):
        raw = dot(normed_ref[...], whole(g), ((1,), (0,)))
        return raw.astype(BF16).astype(F32)

    first_hop(0)
    first_hop(1)
    for direction in (1, -1):
        tok_ship(direction, 1)
    tok_across(0)
    first_hop(2)
    first_hop(3)
    relay_on(1)
    for copy in small:
        copy.wait()
    startt[...] = start_v[0].T.reshape(startt.shape)

    first_wait(0)
    pass_on(1, 0)
    first_wait(1)
    pass_on(1, 1)
    first_wait(2)
    pass_on(1, 2)
    relay_on(2)
    for k in range(1, nkx):
        for direction in (1, -1):
            tok_wait(direction, k)
            tok_ship(direction, k + 1)
            tok_across(-direction * k)
    pass_on(2, 0, 1)
    relay_on(3)
    first_wait(3)
    pass_on(2, 2)
    pass_on(1, 3)
    for direction in (1, -1):
        tok_wait(direction, nkx)
    tok_across(nkx)
    pass_on(3, 0, 1)
    relay_on(4)
    pass_on(3, 2)
    for offset in range(nx):
        tok_across_wait(offset)
    tokens_f = tok[...].reshape(rows, tok.shape[-1]).astype(F32)
    scale = lax.rsqrt(jnp.mean(tokens_f * tokens_f, axis=-1, keepdims=True) + EPS)
    normed_ref[...] = (tokens_f * scale * gain_v[...]).astype(BF16)
    pass_on(4, 0, 1)
    relay_done()
    pass_on(4, 2)
    pass_on(1, 4, 5)
    pass_on(2, 3)

    row = lax.broadcasted_iota(jnp.int32, (BLOCK, BLOCK), 0)
    col = lax.broadcasted_iota(jnp.int32, (BLOCK, BLOCK), 1)
    causal = row >= col
    lower = causal.astype(F32)

    done(0)
    raw = project(0)
    write_in = gap_v[...] * jax.nn.sigmoid(-raw)
    log_keep = jnp.log1p(-write_in)
    w_ref[...] = write_in
    done(1)
    u_ref[...] = project(1)
    memory = None
    total = jnp.zeros((1, dk), F32)
    for b in range(blocks):
        at = pl.ds(b * BLOCK, BLOCK)
        lk = log_keep[b * BLOCK : (b + 1) * BLOCK]
        extra = jnp.where(causal, extra_v[:, at], 0.0)
        running = dot(lower, lk, ((1,), (0,)), HIGHEST) + jnp.sum(extra, axis=1, keepdims=True)
        r_ref[at] = running
        final = running[BLOCK - 1 :]
        off_ref[pl.ds(b, 1)] = total
        total = total + final
        weighted = w_ref[at] * jnp.exp(final - running)
        fresh = dot(u_ref[at], weighted, ((0,), (0,)), HIGHEST)
        if memory is None:
            lprev[b] = jnp.zeros_like(fresh)
            memory = fresh
        else:
            lprev[b] = memory
            memory = memory * jnp.exp(final) + fresh
    ysend[:, pl.ds(0, vrows)] = memory.reshape(ny, vrows, dk)
    ysend[:, pl.ds(vrows, 8)] = jnp.broadcast_to(total[None], (ny, 8, dk))
    yrecv[y] = ysend[y]
    msg = pl.ds(0, vrows + 1)
    for d in far_first:
        to = lax.rem(y + d, ny)
        remote(ysend.at[to, msg], yrecv.at[y, msg], st_send.at[0], st_recv.at[0], {Y: to}).start()
    pass_on(2, 4, 5)
    pass_on(3, 3)

    done(2)
    raw = project(2)
    queries = silu(raw[:, :dk])
    gate_out = silu(raw[:, dk:])
    landed(yrecv.at[pl.ds(0, ny - 1), msg], st_recv.at[0])
    so_far = jnp.zeros((vrows, dk), F32)
    logs = jnp.zeros((1, dk), F32)
    for j in range(ny):
        pref[j] = so_far
        dec[pl.ds(j, 1)] = logs
        step = yrecv[j, pl.ds(vrows, 1)]
        so_far = so_far * jnp.exp(step) + yrecv[j, pl.ds(0, vrows)]
        logs = logs + step
    zbuf[z, pl.ds(0, vrows)] = so_far
    zbuf[z, pl.ds(vrows, 8)] = jnp.broadcast_to(logs, (8, dk))
    for d in far_first:
        ref = zbuf.at[z, msg]
        remote(ref, ref, st_send.at[1], st_recv.at[1], {Z: lax.rem(z + d, nz)}).start()
    pass_on(3, 4, 5)
    pass_on(4, 3)

    local, lifted = [], []
    for b in range(blocks):
        at = pl.ds(b * BLOCK, BLOCK)
        running = r_ref[at]
        mid = running[BLOCK // 2 - 1 : BLOCK // 2]
        q = queries[b * BLOCK : (b + 1) * BLOCK]
        scores = dot(
            q * jnp.exp(running - mid), w_ref[at] * jnp.exp(mid - running), ((1,), (1,)), HIGHEST
        )
        scores = jnp.where(causal, scores, 0.0)
        here = dot(scores, u_ref[at], ((1,), (0,)), HIGHEST)
        here = here + dot(q * jnp.exp(running), lprev[b], ((1,), (1,)), HIGHEST)
        local.append(here)
        lifted.append(q * jnp.exp(running + off_ref[pl.ds(b, 1)]))
    local = jnp.concatenate(local, axis=0)
    lifted = jnp.concatenate(lifted, axis=0)

    per = rows // (nx * nc)
    pass_on(4, 4)
    done(3)
    raw = project(3)
    gated = raw[:, :dk] * raw[:, dk:]
    gext[pl.ds(8, rows)] = gated
    halo_send[...] = gated[rows - 8 :]
    pass_on(4, 5)
    ship(halo_send, gext.at[pl.ds(0, 8)], st_send.at[3], st_recv.at[3], after)

    landed(zbuf.at[pl.ds(0, nz - 1), msg], st_recv.at[1])
    carry = startt[y]
    for j in range(nz):
        later = carry * jnp.exp(zbuf[j, pl.ds(vrows, 1)]) + zbuf[j, pl.ds(0, vrows)]
        carry = jnp.where(j < z, later, carry)
    for j in range(ny):
        back_send[j] = carry * jnp.exp(dec[pl.ds(j, 1)]) + pref[j]
    back_recv[y] = back_send[y]
    for d in far_first:
        to = lax.rem(y + d, ny)
        remote(back_send.at[to], back_recv.at[y], st_send.at[2], st_recv.at[2], {Y: to}).start()

    done(4)
    outer = project(4)
    landed(back_recv.at[pl.ds(0, ny - 1)], st_recv.at[2])
    carried = back_recv[...].reshape(dk, dk)
    mixed = local + dot(lifted, carried, ((1,), (1,)), HIGHEST)
    norm = lax.rsqrt(jnp.mean(mixed * mixed, axis=-1, keepdims=True) + EPS)
    rec = (mixed * norm * sgain_v[...] * gate_out).astype(BF16)
    both[:, :, :, pl.ds(0, dk)] = rec.reshape(nx, nc, per, dk)

    landed(gext.at[pl.ds(0, 8)], st_recv.at[3])
    first = jnp.logical_and(z == 0, y == 0)
    halo = jnp.where(first, 0.0, gext[pl.ds(0, 8)])
    gext[pl.ds(0, 8)] = halo
    conv = (
        taps_v[pl.ds(0, 1)] * gext[pl.ds(6, rows)]
        + taps_v[pl.ds(1, 1)] * gext[pl.ds(7, rows)]
        + taps_v[pl.ds(2, 1)] * gext[pl.ds(8, rows)]
    )
    short = (outer * conv).astype(BF16)
    both[:, :, :, pl.ds(dk, dk)] = short.reshape(nx, nc, per, dk)
    done(5)

    weights = whole(5)
    width = out.shape[1]
    chunks = 4
    size = width // chunks
    theirs = both[:, 1 - c].reshape(nx * per, 2 * dk)
    mine = both[:, c].reshape(nx * per, 2 * dk)

    def pair_ship(q):
        at = pl.ds(q * size, size)
        remote(psend.at[:, :, at], precv.at[:, :, at], pd_send, pd_recv.at[q], {C: 1 - c}).start()

    own = []
    for q in range(chunks):
        part = dot(theirs, weights[q * size : (q + 1) * size], ((1,), (1,)))
        psend[:, :, pl.ds(q * size, size)] = part.astype(BF16).reshape(nx, per, size)
        own.append(dot(mine, weights[q * size : (q + 1) * size], ((1,), (1,))))
        pair_ship(q)

    part = size // 2
    ways = ((0, lax.rem(x + 1, nx)), (1, lax.rem(x + nx - 1, nx)))
    opposite = lax.rem(x + nx // 2, nx)
    relays = nx == 4

    def hop(src, dst, q, kind, d, to):
        remote(src, dst, px_send, px_recv.at[q, kind, d], {X: to}).start()

    def cols(q, d):
        return pl.ds(q * size + d * part, part)

    def push_far(q):
        if relays:
            for d, to in ways:
                hop(ssum.at[opposite, :, cols(q, d)], xrelay.at[:, cols(q, d)], q, 0, d, to)

    def push(q):
        for d, to in ways:
            hop(ssum.at[to, :, cols(q, 1 - d)], xrecv.at[d, :, cols(q, 1 - d)], q, 1, d, to)

    def push_added(q):
        for d, to in ways:
            hop(ssum.at[to, :, cols(q, d)], xrecv.at[d, :, cols(q, d)], q, 2, d, to)

    for q in range(chunks):
        at = pl.ds(q * size, size)
        landed(precv.at[:, :, at], pd_recv.at[q])
        mix = own[q].reshape(nx, per, size) + precv[:, :, at].astype(F32)
        ssum[:, :, at] = mix.astype(BF16)
        if q > 0:
            push_far(q - 1)
    push_far(chunks - 1)
    for q in range(chunks):
        push(q)
    if relays:
        for q in range(chunks):
            for d, to in ways:
                landed(xrelay.at[:, cols(q, d)], px_recv.at[q, 0, d])
                added = ssum[to, :, cols(q, d)].astype(F32) + xrelay[:, cols(q, d)].astype(F32)
                ssum[to, :, cols(q, d)] = added.astype(BF16)
            if q > 0:
                push_added(q - 1)
        push_added(chunks - 1)
    for q in range(chunks):
        at = pl.ds(q * size, size)
        acc = ssum[x, :, at].astype(F32)
        for d, to in ways:
            landed(xrecv.at[d, :, cols(q, 1 - d)], px_recv.at[q, 1, d])
            if relays:
                landed(xrecv.at[d, :, cols(q, d)], px_recv.at[q, 2, d])
        if relays:
            acc = acc + xrecv[0, :, at].astype(F32) + xrecv[1, :, at].astype(F32)
        else:
            ways_back = [xrecv[1 - h, :, cols(q, h)].astype(F32) for h in range(2)]
            acc = acc + jnp.concatenate(ways_back, axis=1)
        out[:, at] = acc.astype(BF16)

    for g in range(6):
        left(groups[g].at[pl.ds(0, n - 1), 0], p1_send.at[g])
        left(groups[g].at[pl.ds(0, n - 1)], r_send.at[g])
    left(ysend.at[pl.ds(0, ny - 1), msg], st_send.at[0])
    left(zbuf.at[pl.ds(0, nz - 1), msg], st_send.at[1])
    left(back_send.at[pl.ds(0, ny - 1)], st_send.at[2])
    left(psend, pd_send)
    left(ssum.at[pl.ds(0, nx - 1)], px_send)
    for copy in pending:
        copy.wait_send()


def on_device(sizes, *args):
    (
        tokens,
        norm_gain,
        w_query,
        w_forget,
        w_input,
        w_outgate,
        w_bgate,
        w_cgate,
        w_value,
        floor_gap,
        extra_decay,
        start_state,
        state_gain,
        conv_taps,
        out_rec,
        out_conv,
    ) = args
    nz, ny, nx, nc = sizes
    per, model = tokens.shape
    rows = per * nx * nc
    blocks = rows // BLOCK
    dk = floor_gap.shape[1]
    half = per // 2
    vrows = dk // ny
    vmem = pl.BlockSpec(memory_space=pltpu.VMEM)
    hbm = pl.BlockSpec(memory_space=pl.ANY)
    dma = pltpu.SemaphoreType.DMA
    steps = nz // 2
    gathered = [(nz, ny, 2, half, k * dk) for k in (1, 1, 2, 2, 1, 2)]
    operands = (
        tokens,
        norm_gain[None],
        w_query,
        w_forget,
        w_input,
        w_outgate,
        w_bgate,
        w_cgate,
        w_value,
        floor_gap,
        extra_decay.T,
        start_state,
        state_gain[None],
        conv_taps,
        out_rec.T,
        out_conv.T,
    )
    small = (1, 9, 10, 11, 12, 13)
    scratch = [
        pltpu.VMEM((nx, nc, per, model), BF16),
        *[pltpu.VMEM(shape, BF16) for shape in gathered],
        pltpu.VMEM((rows, model), BF16),
        pltpu.VMEM((blocks, dk), F32),
        pltpu.VMEM((rows, dk), F32),
        pltpu.VMEM((rows, dk), F32),
        pltpu.VMEM((rows, dk), F32),
        pltpu.VMEM((blocks, dk, dk), F32),
        pltpu.VMEM((ny, vrows, dk), F32),
        pltpu.VMEM((ny, vrows + 8, dk), F32),
        pltpu.VMEM((ny, vrows + 8, dk), F32),
        pltpu.VMEM((nz, vrows + 8, dk), F32),
        pltpu.VMEM((ny, vrows, dk), F32),
        pltpu.VMEM((ny, dk), F32),
        pltpu.VMEM((ny, vrows, dk), F32),
        pltpu.VMEM((ny, vrows, dk), F32),
        pltpu.VMEM((8, dk), F32),
        pltpu.VMEM((rows + 8, dk), F32),
        pltpu.VMEM((nx, nc, per, 2 * dk), BF16),
        *[pltpu.VMEM((nx, per, model), BF16)] * 3,
        pltpu.VMEM((per, model), BF16),
        pltpu.VMEM((2, per, model), BF16),
        *[pltpu.VMEM(operands[i].shape, F32) for i in small],
        dma((13,)),
        dma((6,)),
        dma((6,)),
        dma((steps, 2)),
        dma((6,)),
        dma((6, steps)),
        dma((2, nx // 2)),
        dma((2, nx // 2)),
        dma((nx,)),
        dma((nx,)),
        dma((4,)),
        dma((4,)),
        dma,
        dma((4,)),
        dma,
        dma((4, 3, 2)),
    ]
    return pl.pallas_call(
        functools.partial(kernel, sizes),
        out_shape=jax.ShapeDtypeStruct((per, model), BF16),
        in_specs=[hbm] * len(operands),
        out_specs=vmem,
        scratch_shapes=scratch,
        compiler_params=pltpu.CompilerParams(collective_id=0, has_side_effects=True),
    )(*operands)


def on_torus(devices, sizes):
    torus = Mesh(devices.reshape(sizes), SP_TP)
    return jax.shard_map(
        functools.partial(on_device, sizes),
        mesh=torus,
        in_specs=(
            P(SP_TP, None),
            P(),
            P(SP, TP),
            P(SP, TP),
            P(SP, TP),
            P(SP, TP),
            P(SP, TP),
            P(SP, TP),
            P(SP, TP),
            P(TP, None),
            P(SP, TP),
            P(TP, None, None),
            P(),
            P(None, TP),
            P(TP, SP),
            P(TP, SP),
        ),
        out_specs=P(SP_TP, None),
        check_vma=False,
    )


def solution(mesh):
    return on_torus(mesh.devices, (8, 8, 4, 2))
```

```python
import functools

import jax
import jax.numpy as jnp
from jax import lax
from jax.experimental import pallas as pl
from jax.experimental.pallas import tpu as pltpu
from jax.sharding import Mesh
from jax.sharding import PartitionSpec as P

BLOCK = 64
Z, Y, X, C = "sp_0", "sp_1", "tp_0", "tp_1"
SP = (Z, Y)
TP = (X, C)
SP_TP = (Z, Y, X, C)
MESH = pl.DeviceIdType.MESH
EPS = 1e-06
HIGHEST = lax.Precision.HIGHEST
F32 = jnp.float32
BF16 = jnp.bfloat16


def dot(a, b, dims, precision=None):
    return lax.dot_general(a, b, (dims, ((), ())), precision=precision, preferred_element_type=F32)


def silu(v):
    return v * jax.nn.sigmoid(v)


def kernel(
    sizes,
    tokens,
    gain,
    w_query,
    w_forget,
    w_input,
    w_outgate,
    w_bgate,
    w_cgate,
    w_value,
    floor_gap,
    extra_decay,
    start_state,
    state_gain,
    taps,
    rec_t,
    conv_t,
    out,
    tok,
    wg0,
    wg1,
    wg2,
    wg3,
    wg4,
    wg5,
    normed_ref,
    off_ref,
    r_ref,
    u_ref,
    w_ref,
    lprev,
    startt,
    ysend,
    yrecv,
    ydec,
    zbuf,
    zdec,
    pref,
    dec,
    back_send,
    back_recv,
    halo_send,
    gext,
    both,
    psend,
    precv,
    ssum,
    xrelay,
    xrecv,
    gain_v,
    gap_v,
    extra_v,
    start_v,
    sgain_v,
    taps_v,
    load_sem,
    p1_send,
    p1_recv,
    p1r_recv,
    r_send,
    r_recv,
    tx_send,
    tx_recv,
    td_send,
    td_recv,
    st_send,
    st_recv,
    pd_send,
    pd_recv,
    px_send,
    px_recv,
):
    nz, ny, nx, nc = sizes
    n = nz
    z, y, x, c = (lax.axis_index(name) for name in (Z, Y, X, C))
    groups = (wg0, wg1, wg2, wg3, wg4, wg5)
    sources = (
        (w_forget,),
        (w_input,),
        (w_cgate, w_value),
        (w_query, w_outgate),
        (w_bgate,),
        (rec_t, conv_t),
    )
    half = tokens.shape[0] // 2
    rows = nx * nc * tokens.shape[0]
    blocks = rows // BLOCK
    dk = floor_gap.shape[1]
    vrows = dk // ny

    wrap = jnp.where(y == ny - 1, 1, 0)
    unwrap = jnp.where(y == 0, 1, 0)
    after = {Z: lax.rem(z + wrap, nz), Y: lax.rem(y + 1, ny)}
    before = {Z: lax.rem(z + nz - unwrap, nz), Y: lax.rem(y + ny - 1, ny)}
    far_first = sorted(range(1, n), key=lambda d: -min(d, n - d))
    peers = [{Y: lax.rem(y + d, ny)} for d in far_first]
    peers += [{Z: lax.rem(z + d, nz)} for d in far_first]
    peers += [{X: lax.rem(x + d, nx)} for d in range(1, nx)]
    peers += [{C: 1 - c}, after, before]
    barrier = pltpu.get_barrier_semaphore()
    for peer in peers:
        pl.semaphore_signal(barrier, inc=1, device_id=peer, device_id_type=MESH)

    tok_load = pltpu.make_async_copy(tokens, tok.at[x, c], load_sem.at[6])

    def load(g):
        lo = 0
        for part in sources[g]:
            width = part.shape[1]
            for h in range(2):
                pltpu.make_async_copy(
                    part.at[pl.ds(h * half, half)],
                    groups[g].at[z, y, h, :, pl.ds(lo, width)],
                    load_sem.at[g],
                ).start()
            lo += width

    def wait_load(g):
        ref = groups[g].at[z, y]
        pltpu.make_async_copy(ref, ref, load_sem.at[g]).wait()

    load(0)
    load(1)
    tok_load.start()
    for g in range(2, 6):
        load(g)
    small = [
        pltpu.make_async_copy(src, dst, load_sem.at[7 + i])
        for i, (src, dst) in enumerate(
            (
                (gain, gain_v),
                (floor_gap, gap_v),
                (extra_decay, extra_v),
                (start_state, start_v),
                (state_gain, sgain_v),
                (taps, taps_v),
            )
        )
    ]
    for copy in small:
        copy.start()
    for g in range(6):
        wait_load(g)
    tok_load.wait()
    pl.semaphore_wait(barrier, len(peers))

    def remote(src, dst, send, recv, to):
        return pltpu.make_async_remote_copy(
            src_ref=src, dst_ref=dst, send_sem=send, recv_sem=recv, device_id=to, device_id_type=MESH
        )

    pending = []

    def ship(src, dst, send, recv, to):
        copy = remote(src, dst, send, recv, to)
        copy.start()
        pending.append(copy)

    def landed(ref, recv):
        remote(ref, ref, recv, recv, {C: 1 - c}).wait_recv()

    def left(ref, send):
        remote(ref, ref, send, send, {C: 1 - c}).wait_send()

    nkx = nx // 2

    def tok_part(index, direction, k):
        if k < nkx:
            return tok.at[index, c]
        return tok.at[index, c, pl.ds(0 if direction > 0 else half, half)]

    def tok_ship(direction, k):
        ref = tok_part(lax.rem(x - direction * (k - 1) + nx, nx), direction, k)
        d = 0 if direction > 0 else 1
        to = {X: lax.rem(x + direction + nx, nx)}
        ship(ref, ref, tx_send.at[d, k - 1], tx_recv.at[d, k - 1], to)

    def tok_wait(direction, k):
        d = 0 if direction > 0 else 1
        landed(tok_part(lax.rem(x - direction * k + nx, nx), direction, k), tx_recv.at[d, k - 1])

    def tok_across(offset):
        ref = tok.at[lax.rem(x + offset + nx, nx), c]
        ship(ref, ref, td_send.at[offset % nx], td_recv.at[offset % nx], {C: 1 - c})

    def tok_across_wait(offset):
        landed(tok.at[lax.rem(x + offset + nx, nx), 1 - c], td_recv.at[offset % nx])

    lines = ((Y, y), (Z, z))

    def first_hop(g):
        for color, (axis, me) in enumerate(lines):
            ref = groups[g].at[z, y, color]
            for d in far_first:
                remote(
                    ref, ref, p1_send.at[g], p1_recv.at[g], {axis: lax.rem(me + d, n)}
                ).start()

    def first_wait(g):
        landed(groups[g].at[pl.ds(0, n - 1), 0], p1_recv.at[g])

    relayed = (4, 5)
    steps = n // 2

    def relay_ship(k):
        for color, (axis, me) in enumerate(lines):
            for direction in (1, -1):
                index = lax.rem(me - direction * (k - 1) + n, n)
                to = {axis: lax.rem(me + direction + n, n)}
                for g in relayed:
                    if k == steps and (g == 4) == (direction > 0):
                        continue
                    w = groups[g]
                    ref = w.at[z, index, 0] if color == 0 else w.at[index, y, 1]
                    remote(ref, ref, p1_send.at[g], p1r_recv.at[k - 1, g - 4], to).start()

    def relay_wait(k):
        for g in relayed:
            landed(groups[g].at[pl.ds(0, 2 if k < steps else 1), 0], p1r_recv.at[k - 1, g - 4])

    relay = [0, 0]

    def relay_seen(k):
        while relay[1] < k:
            relay[1] += 1
            relay_wait(relay[1])

    def relay_on(k):
        while relay[0] < min(k, steps):
            relay_seen(relay[0])
            relay[0] += 1
            relay_ship(relay[0])

    def relay_done():
        relay_on(steps)
        relay_seen(steps)

    rings = ((Z, z), (Y, y))

    def ring_ship(g, k):
        w = groups[g]
        for color, (axis, me) in enumerate(rings):
            for direction in (1, -1):
                index = lax.rem(me - direction * (k - 1) + n, n)
                if k == steps:
                    part = pl.ds(0 if direction > 0 else n // 2, n // 2)
                else:
                    part = pl.ds(0, n)
                ref = w.at[index, part, 0] if color == 0 else w.at[part, index, 1]
                to = {axis: lax.rem(me + direction + n, n)}
                remote(ref, ref, r_send.at[g], r_recv.at[g, k - 1], to).start()

    def ring_wait(g, k):
        landed(groups[g].at[pl.ds(0, 2 if k < steps else 1)], r_recv.at[g, k - 1])

    sent, seen = [0] * 6, [0] * 6

    def see(g, k):
        while seen[g] < k:
            seen[g] += 1
            ring_wait(g, seen[g])

    def pass_on(k, *which):
        for g in which:
            while sent[g] < min(k, steps):
                see(g, sent[g])
                sent[g] += 1
                ring_ship(g, sent[g])

    def done(g):
        pass_on(steps, g)
        see(g, steps)

    def whole(g):
        w = groups[g][...]
        return w.reshape(-1, w.shape[-1])

    def project(g):
        raw = dot(normed_ref[...], whole(g), ((1,), (0,)))
        return raw.astype(BF16).astype(F32)

    first_hop(0)
    first_hop(1)
    for direction in (1, -1):
        tok_ship(direction, 1)
    tok_across(0)
    first_hop(2)
    first_hop(3)
    relay_on(1)
    for copy in small:
        copy.wait()
    startt[...] = start_v[0].T.reshape(startt.shape)

    first_wait(0)
    pass_on(1, 0)
    first_wait(1)
    pass_on(1, 1)
    first_wait(2)
    pass_on(1, 2)
    relay_on(2)
    for k in range(1, nkx):
        for direction in (1, -1):
            tok_wait(direction, k)
            tok_ship(direction, k + 1)
            tok_across(-direction * k)
    pass_on(2, 0, 1)
    relay_on(3)
    pass_on(2, 2)
    for direction in (1, -1):
        tok_wait(direction, nkx)
    tok_across(nkx)
    pass_on(3, 0, 1)
    relay_on(4)
    pass_on(3, 2)
    for offset in range(nx):
        tok_across_wait(offset)
    tokens_f = tok[...].reshape(rows, tok.shape[-1]).astype(F32)
    scale = lax.rsqrt(jnp.mean(tokens_f * tokens_f, axis=-1, keepdims=True) + EPS)
    normed_ref[...] = (tokens_f * scale * gain_v[...]).astype(BF16)
    pass_on(4, 0, 1)
    first_wait(3)
    pass_on(1, 3)
    relay_done()
    pass_on(4, 2)
    pass_on(1, 4, 5)

    row = lax.broadcasted_iota(jnp.int32, (BLOCK, BLOCK), 0)
    col = lax.broadcasted_iota(jnp.int32, (BLOCK, BLOCK), 1)
    causal = row >= col
    lower = causal.astype(F32)

    done(0)
    raw = project(0)
    write_in = gap_v[...] * jax.nn.sigmoid(-raw)
    log_keep = jnp.log1p(-write_in)
    w_ref[...] = write_in
    done(1)
    u_ref[...] = project(1)
    memory = None
    total = jnp.zeros((1, dk), F32)
    for b in range(blocks):
        at = pl.ds(b * BLOCK, BLOCK)
        lk = log_keep[b * BLOCK : (b + 1) * BLOCK]
        extra = jnp.where(causal, extra_v[:, at], 0.0)
        running = dot(lower, lk, ((1,), (0,)), HIGHEST) + jnp.sum(extra, axis=1, keepdims=True)
        r_ref[at] = running
        final = running[BLOCK - 1 :]
        off_ref[pl.ds(b, 1)] = total
        total = total + final
        weighted = w_ref[at] * jnp.exp(final - running)
        fresh = dot(u_ref[at], weighted, ((0,), (0,)), HIGHEST)
        if memory is None:
            lprev[b] = jnp.zeros_like(fresh)
            memory = fresh
        else:
            lprev[b] = memory
            memory = memory * jnp.exp(final) + fresh
    ysend[...] = memory.reshape(ny, vrows, dk).astype(BF16)
    ydec[y] = jnp.broadcast_to(total, (8, dk))
    yrecv[y] = ysend[y]
    line = pl.ds(0, 1)
    for d in far_first:
        to = lax.rem(y + d, ny)
        remote(ysend.at[to], yrecv.at[y], st_send.at[0], st_recv.at[0], {Y: to}).start()
        ref = ydec.at[y, line]
        remote(ref, ref, st_send.at[4], st_recv.at[4], {Y: to}).start()
    pass_on(2, 3, 4, 5)

    per = rows // (nx * nc)
    done(2)
    raw = project(2)
    gated = raw[:, :dk] * raw[:, dk:]
    gext[pl.ds(8, rows)] = gated
    halo_send[...] = gated[rows - 8 :]

    landed(yrecv.at[pl.ds(0, ny - 1)], st_recv.at[0])
    landed(ydec.at[pl.ds(0, ny - 1), line], st_recv.at[4])
    so_far = jnp.zeros((vrows, dk), F32)
    logs = jnp.zeros((1, dk), F32)
    for j in range(ny):
        pref[j] = so_far
        dec[pl.ds(j, 1)] = logs
        step = ydec[j, line]
        so_far = so_far * jnp.exp(step) + yrecv[j].astype(F32)
        logs = logs + step
    zbuf[z] = so_far.astype(BF16)
    zdec[z] = jnp.broadcast_to(logs, (8, dk))
    for d in far_first:
        for k, ref in ((1, zbuf.at[z]), (5, zdec.at[z, line])):
            remote(ref, ref, st_send.at[k], st_recv.at[k], {Z: lax.rem(z + d, nz)}).start()
    ship(halo_send, gext.at[pl.ds(0, 8)], st_send.at[3], st_recv.at[3], after)
    pass_on(3, 3, 4, 5)
    pass_on(4, 3, 4)

    landed(zbuf.at[pl.ds(0, nz - 1)], st_recv.at[1])
    landed(zdec.at[pl.ds(0, nz - 1), line], st_recv.at[5])
    carry = startt[y]
    for j in range(nz):
        later = carry * jnp.exp(zdec[j, line]) + zbuf[j].astype(F32)
        carry = jnp.where(j < z, later, carry)
    for j in range(ny):
        back_send[j] = (carry * jnp.exp(dec[pl.ds(j, 1)]) + pref[j]).astype(BF16)
    back_recv[y] = back_send[y]
    for d in far_first:
        to = lax.rem(y + d, ny)
        remote(back_send.at[to], back_recv.at[y], st_send.at[2], st_recv.at[2], {Y: to}).start()

    pass_on(4, 5)
    landed(gext.at[pl.ds(0, 8)], st_recv.at[3])
    first = jnp.logical_and(z == 0, y == 0)
    halo = jnp.where(first, 0.0, gext[pl.ds(0, 8)])
    gext[pl.ds(0, 8)] = halo
    conv = (
        taps_v[pl.ds(0, 1)] * gext[pl.ds(6, rows)]
        + taps_v[pl.ds(1, 1)] * gext[pl.ds(7, rows)]
        + taps_v[pl.ds(2, 1)] * gext[pl.ds(8, rows)]
    )
    done(3)
    raw = project(3)
    queries = silu(raw[:, :dk])
    gate_out = silu(raw[:, dk:])
    local, lifted = [], []
    for b in range(blocks):
        at = pl.ds(b * BLOCK, BLOCK)
        running = r_ref[at]
        mid = running[BLOCK // 2 - 1 : BLOCK // 2]
        q = queries[b * BLOCK : (b + 1) * BLOCK]
        scores = dot(
            q * jnp.exp(running - mid), w_ref[at] * jnp.exp(mid - running), ((1,), (1,)), HIGHEST
        )
        scores = jnp.where(causal, scores, 0.0)
        here = dot(scores, u_ref[at], ((1,), (0,)), HIGHEST)
        here = here + dot(q * jnp.exp(running), lprev[b], ((1,), (1,)), HIGHEST)
        local.append(here)
        lifted.append(q * jnp.exp(running + off_ref[pl.ds(b, 1)]))
    local = jnp.concatenate(local, axis=0)
    lifted = jnp.concatenate(lifted, axis=0)

    done(4)
    short = (project(4) * conv).astype(BF16)
    both[:, :, :, pl.ds(dk, dk)] = short.reshape(nx, nc, per, dk)
    landed(back_recv.at[pl.ds(0, ny - 1)], st_recv.at[2])
    carried = back_recv[...].reshape(dk, dk).astype(F32)
    mixed = local + dot(lifted, carried, ((1,), (1,)), HIGHEST)
    norm = lax.rsqrt(jnp.mean(mixed * mixed, axis=-1, keepdims=True) + EPS)
    rec = (mixed * norm * sgain_v[...] * gate_out).astype(BF16)
    both[:, :, :, pl.ds(0, dk)] = rec.reshape(nx, nc, per, dk)

    done(5)

    weights = whole(5)
    width = out.shape[1]
    chunks = 4
    size = width // chunks
    theirs = both[:, 1 - c].reshape(nx * per, 2 * dk)
    mine = both[:, c].reshape(nx * per, 2 * dk)

    def pair_ship(q):
        at = pl.ds(q * size, size)
        remote(psend.at[:, :, at], precv.at[:, :, at], pd_send, pd_recv.at[q], {C: 1 - c}).start()

    for q in range(chunks):
        part = dot(theirs, weights[q * size : (q + 1) * size], ((1,), (1,)))
        psend[:, :, pl.ds(q * size, size)] = part.astype(BF16).reshape(nx, per, size)
        if q > 0:
            pair_ship(q - 1)
    own = [dot(mine, weights[:size], ((1,), (1,)))]
    pair_ship(chunks - 1)

    part = size // 2
    ways = ((0, lax.rem(x + 1, nx)), (1, lax.rem(x + nx - 1, nx)))
    opposite = lax.rem(x + nx // 2, nx)
    relays = nx == 4

    def hop(src, dst, q, kind, d, to):
        remote(src, dst, px_send, px_recv.at[q, kind, d], {X: to}).start()

    def cols(q, d):
        return pl.ds(q * size + d * part, part)

    def push_far(q):
        if relays:
            for d, to in ways:
                hop(ssum.at[opposite, :, cols(q, d)], xrelay.at[:, cols(q, d)], q, 0, d, to)

    def push(q):
        for d, to in ways:
            hop(ssum.at[to, :, cols(q, 1 - d)], xrecv.at[d, :, cols(q, 1 - d)], q, 1, d, to)

    def push_added(q, way):
        d, to = way
        hop(ssum.at[to, :, cols(q, d)], xrecv.at[d, :, cols(q, d)], q, 2, d, to)

    for q in range(chunks):
        at = pl.ds(q * size, size)
        landed(precv.at[:, :, at], pd_recv.at[q])
        mix = own[q].reshape(nx, per, size) + precv[:, :, at].astype(F32)
        ssum[:, :, at] = mix.astype(BF16)
        if q < chunks - 1:
            own.append(dot(mine, weights[(q + 1) * size : (q + 2) * size], ((1,), (1,))))
        push_far(q)
    for q in range(chunks):
        push(q)
    if relays:
        held = None
        for q in range(chunks):
            for way in ways:
                d, to = way
                landed(xrelay.at[:, cols(q, d)], px_recv.at[q, 0, d])
                added = ssum[to, :, cols(q, d)].astype(F32) + xrelay[:, cols(q, d)].astype(F32)
                ssum[to, :, cols(q, d)] = added.astype(BF16)
                if held is not None:
                    push_added(*held)
                held = (q, way)
        push_added(*held)
    for q in range(chunks):
        at = pl.ds(q * size, size)
        acc = ssum[x, :, at].astype(F32)
        for d, to in ways:
            landed(xrecv.at[d, :, cols(q, 1 - d)], px_recv.at[q, 1, d])
            if relays:
                landed(xrecv.at[d, :, cols(q, d)], px_recv.at[q, 2, d])
        if relays:
            acc = acc + xrecv[0, :, at].astype(F32) + xrecv[1, :, at].astype(F32)
        else:
            ways_back = [xrecv[1 - h, :, cols(q, h)].astype(F32) for h in range(2)]
            acc = acc + jnp.concatenate(ways_back, axis=1)
        out[:, at] = acc.astype(BF16)

    for g in range(6):
        left(groups[g].at[pl.ds(0, n - 1), 0], p1_send.at[g])
        left(groups[g].at[pl.ds(0, n - 1)], r_send.at[g])
    left(ysend.at[pl.ds(0, ny - 1)], st_send.at[0])
    left(ydec.at[pl.ds(0, ny - 1), line], st_send.at[4])
    left(zbuf.at[pl.ds(0, nz - 1)], st_send.at[1])
    left(zdec.at[pl.ds(0, nz - 1), line], st_send.at[5])
    left(back_send.at[pl.ds(0, ny - 1)], st_send.at[2])
    left(psend, pd_send)
    left(ssum.at[pl.ds(0, nx - 1)], px_send)
    for copy in pending:
        copy.wait_send()


def on_device(sizes, *args):
    (
        tokens,
        norm_gain,
        w_query,
        w_forget,
        w_input,
        w_outgate,
        w_bgate,
        w_cgate,
        w_value,
        floor_gap,
        extra_decay,
        start_state,
        state_gain,
        conv_taps,
        out_rec,
        out_conv,
    ) = args
    nz, ny, nx, nc = sizes
    per, model = tokens.shape
    rows = per * nx * nc
    blocks = rows // BLOCK
    dk = floor_gap.shape[1]
    half = per // 2
    vrows = dk // ny
    vmem = pl.BlockSpec(memory_space=pltpu.VMEM)
    hbm = pl.BlockSpec(memory_space=pl.ANY)
    dma = pltpu.SemaphoreType.DMA
    steps = nz // 2
    gathered = [(nz, ny, 2, half, k * dk) for k in (1, 1, 2, 2, 1, 2)]
    operands = (
        tokens,
        norm_gain[None],
        w_query,
        w_forget,
        w_input,
        w_outgate,
        w_bgate,
        w_cgate,
        w_value,
        floor_gap,
        extra_decay.T,
        start_state,
        state_gain[None],
        conv_taps,
        out_rec.T,
        out_conv.T,
    )
    small = (1, 9, 10, 11, 12, 13)
    scratch = [
        pltpu.VMEM((nx, nc, per, model), BF16),
        *[pltpu.VMEM(shape, BF16) for shape in gathered],
        pltpu.VMEM((rows, model), BF16),
        pltpu.VMEM((blocks, dk), F32),
        pltpu.VMEM((rows, dk), F32),
        pltpu.VMEM((rows, dk), F32),
        pltpu.VMEM((rows, dk), F32),
        pltpu.VMEM((blocks, dk, dk), F32),
        pltpu.VMEM((ny, vrows, dk), F32),
        pltpu.VMEM((ny, vrows, dk), BF16),
        pltpu.VMEM((ny, vrows, dk), BF16),
        pltpu.VMEM((ny, 8, dk), F32),
        pltpu.VMEM((nz, vrows, dk), BF16),
        pltpu.VMEM((nz, 8, dk), F32),
        pltpu.VMEM((ny, vrows, dk), F32),
        pltpu.VMEM((ny, dk), F32),
        pltpu.VMEM((ny, vrows, dk), BF16),
        pltpu.VMEM((ny, vrows, dk), BF16),
        pltpu.VMEM((8, dk), F32),
        pltpu.VMEM((rows + 8, dk), F32),
        pltpu.VMEM((nx, nc, per, 2 * dk), BF16),
        *[pltpu.VMEM((nx, per, model), BF16)] * 3,
        pltpu.VMEM((per, model), BF16),
        pltpu.VMEM((2, per, model), BF16),
        *[pltpu.VMEM(operands[i].shape, F32) for i in small],
        dma((13,)),
        dma((6,)),
        dma((6,)),
        dma((steps, 2)),
        dma((6,)),
        dma((6, steps)),
        dma((2, nx // 2)),
        dma((2, nx // 2)),
        dma((nx,)),
        dma((nx,)),
        dma((6,)),
        dma((6,)),
        dma,
        dma((4,)),
        dma,
        dma((4, 3, 2)),
    ]
    return pl.pallas_call(
        functools.partial(kernel, sizes),
        out_shape=jax.ShapeDtypeStruct((per, model), BF16),
        in_specs=[hbm] * len(operands),
        out_specs=vmem,
        scratch_shapes=scratch,
        compiler_params=pltpu.CompilerParams(collective_id=0, has_side_effects=True),
    )(*operands)


def on_torus(devices, sizes):
    torus = Mesh(devices.reshape(sizes), SP_TP)
    return jax.shard_map(
        functools.partial(on_device, sizes),
        mesh=torus,
        in_specs=(
            P(SP_TP, None),
            P(),
            P(SP, TP),
            P(SP, TP),
            P(SP, TP),
            P(SP, TP),
            P(SP, TP),
            P(SP, TP),
            P(SP, TP),
            P(TP, None),
            P(SP, TP),
            P(TP, None, None),
            P(),
            P(None, TP),
            P(TP, SP),
            P(TP, SP),
        ),
        out_specs=P(SP_TP, None),
        check_vma=False,
    )


def solution(mesh):
    return on_torus(mesh.devices, (8, 8, 4, 2))
```

```python
import functools

import jax
import jax.numpy as jnp
from jax import lax
from jax.experimental import pallas as pl
from jax.experimental.pallas import tpu as pltpu
from jax.sharding import Mesh
from jax.sharding import PartitionSpec as P

BLOCK = 64
Z, Y, X, C = "sp_0", "sp_1", "tp_0", "tp_1"
SP = (Z, Y)
TP = (X, C)
SP_TP = (Z, Y, X, C)
MESH = pl.DeviceIdType.MESH
EPS = 1e-06
HIGHEST = lax.Precision.HIGHEST
F32 = jnp.float32
BF16 = jnp.bfloat16


def dot(a, b, dims, precision=None):
    return lax.dot_general(a, b, (dims, ((), ())), precision=precision, preferred_element_type=F32)


def silu(v):
    return v * jax.nn.sigmoid(v)


def kernel(
    sizes,
    tokens,
    gain,
    w_query,
    w_forget,
    w_input,
    w_outgate,
    w_bgate,
    w_cgate,
    w_value,
    floor_gap,
    extra_decay,
    start_state,
    state_gain,
    taps,
    rec_t,
    conv_t,
    out,
    tok,
    wg0,
    wg1,
    wg2,
    wg3,
    wg4,
    wg5,
    normed_ref,
    off_ref,
    r_ref,
    u_ref,
    w_ref,
    lprev,
    startt,
    ysend,
    yrecv,
    ydec,
    zbuf,
    zdec,
    pref,
    dec,
    back_send,
    back_recv,
    halo_send,
    gext,
    both,
    psend,
    precv,
    ssum,
    xrelay,
    xrecv,
    gain_v,
    gap_v,
    extra_v,
    start_v,
    sgain_v,
    taps_v,
    load_sem,
    p1_send,
    p1_recv,
    p1r_recv,
    r_send,
    r_recv,
    tx_send,
    tx_recv,
    td_send,
    td_recv,
    st_send,
    st_recv,
    pd_send,
    pd_recv,
    px_send,
    px_recv,
):
    nz, ny, nx, nc = sizes
    n = nz
    z, y, x, c = (lax.axis_index(name) for name in (Z, Y, X, C))
    groups = (wg0, wg1, wg2, wg3, wg4, wg5)
    sources = (
        (w_forget,),
        (w_input,),
        (w_cgate, w_value),
        (w_query, w_outgate),
        (w_bgate,),
        (rec_t, conv_t),
    )
    half = tokens.shape[0] // 2
    rows = nx * nc * tokens.shape[0]
    blocks = rows // BLOCK
    dk = floor_gap.shape[1]
    vrows = dk // ny

    wrap = jnp.where(y == ny - 1, 1, 0)
    unwrap = jnp.where(y == 0, 1, 0)
    after = {Z: lax.rem(z + wrap, nz), Y: lax.rem(y + 1, ny)}
    before = {Z: lax.rem(z + nz - unwrap, nz), Y: lax.rem(y + ny - 1, ny)}
    far_first = sorted(range(1, n), key=lambda d: -min(d, n - d))
    peers = [{Y: lax.rem(y + d, ny)} for d in far_first]
    peers += [{Z: lax.rem(z + d, nz)} for d in far_first]
    peers += [{X: lax.rem(x + d, nx)} for d in range(1, nx)]
    peers += [{C: 1 - c}, after, before]
    barrier = pltpu.get_barrier_semaphore()
    for peer in peers:
        pl.semaphore_signal(barrier, inc=1, device_id=peer, device_id_type=MESH)

    tok_load = pltpu.make_async_copy(tokens, tok.at[x, c], load_sem.at[6])

    def load(g):
        lo = 0
        for part in sources[g]:
            width = part.shape[1]
            for h in range(2):
                pltpu.make_async_copy(
                    part.at[pl.ds(h * half, half)],
                    groups[g].at[z, y, h, :, pl.ds(lo, width)],
                    load_sem.at[g],
                ).start()
            lo += width

    def wait_load(g):
        ref = groups[g].at[z, y]
        pltpu.make_async_copy(ref, ref, load_sem.at[g]).wait()

    load(0)
    load(1)
    tok_load.start()
    for g in range(2, 6):
        load(g)
    small = [
        pltpu.make_async_copy(src, dst, load_sem.at[7 + i])
        for i, (src, dst) in enumerate(
            (
                (gain, gain_v),
                (floor_gap, gap_v),
                (extra_decay, extra_v),
                (start_state, start_v),
                (state_gain, sgain_v),
                (taps, taps_v),
            )
        )
    ]
    for copy in small:
        copy.start()
    for g in range(6):
        wait_load(g)
    tok_load.wait()
    pl.semaphore_wait(barrier, len(peers))

    def remote(src, dst, send, recv, to):
        return pltpu.make_async_remote_copy(
            src_ref=src, dst_ref=dst, send_sem=send, recv_sem=recv, device_id=to, device_id_type=MESH
        )

    pending = []

    def ship(src, dst, send, recv, to):
        copy = remote(src, dst, send, recv, to)
        copy.start()
        pending.append(copy)

    def landed(ref, recv):
        remote(ref, ref, recv, recv, {C: 1 - c}).wait_recv()

    def left(ref, send):
        remote(ref, ref, send, send, {C: 1 - c}).wait_send()

    nkx = nx // 2

    def tok_part(index, direction, k):
        if k < nkx:
            return tok.at[index, c]
        return tok.at[index, c, pl.ds(0 if direction > 0 else half, half)]

    def tok_ship(direction, k):
        ref = tok_part(lax.rem(x - direction * (k - 1) + nx, nx), direction, k)
        d = 0 if direction > 0 else 1
        to = {X: lax.rem(x + direction + nx, nx)}
        ship(ref, ref, tx_send.at[d, k - 1], tx_recv.at[d, k - 1], to)

    def tok_wait(direction, k):
        d = 0 if direction > 0 else 1
        landed(tok_part(lax.rem(x - direction * k + nx, nx), direction, k), tx_recv.at[d, k - 1])

    def tok_across(offset):
        ref = tok.at[lax.rem(x + offset + nx, nx), c]
        ship(ref, ref, td_send.at[offset % nx], td_recv.at[offset % nx], {C: 1 - c})

    def tok_across_wait(offset):
        landed(tok.at[lax.rem(x + offset + nx, nx), 1 - c], td_recv.at[offset % nx])

    lines = ((Y, y), (Z, z))

    def first_hop(g):
        for color, (axis, me) in enumerate(lines):
            ref = groups[g].at[z, y, color]
            for d in far_first:
                remote(
                    ref, ref, p1_send.at[g], p1_recv.at[g], {axis: lax.rem(me + d, n)}
                ).start()

    def first_wait(g):
        landed(groups[g].at[pl.ds(0, n - 1), 0], p1_recv.at[g])

    relayed = (4, 5)
    steps = n // 2

    def relay_ship(k):
        for color, (axis, me) in enumerate(lines):
            for direction in (1, -1):
                index = lax.rem(me - direction * (k - 1) + n, n)
                to = {axis: lax.rem(me + direction + n, n)}
                for g in relayed:
                    if k == steps and (g == 4) == (direction > 0):
                        continue
                    w = groups[g]
                    ref = w.at[z, index, 0] if color == 0 else w.at[index, y, 1]
                    remote(ref, ref, p1_send.at[g], p1r_recv.at[k - 1, g - 4], to).start()

    def relay_wait(k):
        for g in relayed:
            landed(groups[g].at[pl.ds(0, 2 if k < steps else 1), 0], p1r_recv.at[k - 1, g - 4])

    relay = [0, 0]

    def relay_seen(k):
        while relay[1] < k:
            relay[1] += 1
            relay_wait(relay[1])

    def relay_on(k):
        while relay[0] < min(k, steps):
            relay_seen(relay[0])
            relay[0] += 1
            relay_ship(relay[0])

    def relay_done():
        relay_on(steps)
        relay_seen(steps)

    rings = ((Z, z), (Y, y))

    def ring_ship(g, k):
        w = groups[g]
        for color, (axis, me) in enumerate(rings):
            for direction in (1, -1):
                index = lax.rem(me - direction * (k - 1) + n, n)
                if k == steps:
                    part = pl.ds(0 if direction > 0 else n // 2, n // 2)
                else:
                    part = pl.ds(0, n)
                ref = w.at[index, part, 0] if color == 0 else w.at[part, index, 1]
                to = {axis: lax.rem(me + direction + n, n)}
                remote(ref, ref, r_send.at[g], r_recv.at[g, k - 1], to).start()

    def ring_wait(g, k):
        landed(groups[g].at[pl.ds(0, 2 if k < steps else 1)], r_recv.at[g, k - 1])

    sent, seen = [0] * 6, [0] * 6

    def see(g, k):
        while seen[g] < k:
            seen[g] += 1
            ring_wait(g, seen[g])

    def pass_on(k, *which):
        for g in which:
            while sent[g] < min(k, steps):
                see(g, sent[g])
                sent[g] += 1
                ring_ship(g, sent[g])

    def done(g):
        pass_on(steps, g)
        see(g, steps)

    def whole(g):
        w = groups[g][...]
        return w.reshape(-1, w.shape[-1])

    def project(g):
        raw = dot(normed_ref[...], whole(g), ((1,), (0,)))
        return raw.astype(BF16).astype(F32)

    first_hop(0)
    first_hop(1)
    for direction in (1, -1):
        tok_ship(direction, 1)
    tok_across(0)
    first_hop(2)
    first_hop(3)
    relay_on(1)
    for copy in small:
        copy.wait()
    startt[...] = start_v[0].T.reshape(startt.shape)

    first_wait(0)
    pass_on(1, 0)
    first_wait(1)
    pass_on(1, 1)
    first_wait(2)
    pass_on(1, 2)
    relay_on(2)
    for k in range(1, nkx):
        for direction in (1, -1):
            tok_wait(direction, k)
            tok_ship(direction, k + 1)
            tok_across(-direction * k)
    pass_on(2, 0, 1)
    relay_on(3)
    pass_on(2, 2)
    for direction in (1, -1):
        tok_wait(direction, nkx)
    tok_across(nkx)
    pass_on(3, 0, 1)
    relay_on(4)
    pass_on(3, 2)
    for offset in range(nx):
        tok_across_wait(offset)
    tokens_f = tok[...].reshape(rows, tok.shape[-1]).astype(F32)
    scale = lax.rsqrt(jnp.mean(tokens_f * tokens_f, axis=-1, keepdims=True) + EPS)
    normed_ref[...] = (tokens_f * scale * gain_v[...]).astype(BF16)
    pass_on(4, 0, 1)
    first_wait(3)
    pass_on(1, 3)
    relay_done()
    pass_on(4, 2)
    pass_on(1, 4, 5)

    row = lax.broadcasted_iota(jnp.int32, (BLOCK, BLOCK), 0)
    col = lax.broadcasted_iota(jnp.int32, (BLOCK, BLOCK), 1)
    causal = row >= col
    lower = causal.astype(F32)

    done(0)
    raw = project(0)
    write_in = gap_v[...] * jax.nn.sigmoid(-raw)
    log_keep = jnp.log1p(-write_in)
    w_ref[...] = write_in
    done(1)
    u_ref[...] = project(1)
    memory = None
    total = jnp.zeros((1, dk), F32)
    for b in range(blocks):
        at = pl.ds(b * BLOCK, BLOCK)
        lk = log_keep[b * BLOCK : (b + 1) * BLOCK]
        extra = jnp.where(causal, extra_v[:, at], 0.0)
        running = dot(lower, lk, ((1,), (0,)), HIGHEST) + jnp.sum(extra, axis=1, keepdims=True)
        r_ref[at] = running
        final = running[BLOCK - 1 :]
        off_ref[pl.ds(b, 1)] = total
        total = total + final
        weighted = w_ref[at] * jnp.exp(final - running)
        fresh = dot(u_ref[at], weighted, ((0,), (0,)), HIGHEST)
        if memory is None:
            lprev[b] = jnp.zeros_like(fresh)
            memory = fresh
        else:
            lprev[b] = memory
            memory = memory * jnp.exp(final) + fresh
    ysend[...] = memory.reshape(ny, vrows, dk).astype(BF16)
    ydec[y] = jnp.broadcast_to(total, (8, dk))
    yrecv[y] = ysend[y]
    line = pl.ds(0, 1)
    for d in far_first:
        to = lax.rem(y + d, ny)
        remote(ysend.at[to], yrecv.at[y], st_send.at[0], st_recv.at[0], {Y: to}).start()
        ref = ydec.at[y, line]
        remote(ref, ref, st_send.at[4], st_recv.at[4], {Y: to}).start()
    pass_on(2, 3, 4, 5)

    per = rows // (nx * nc)
    done(2)
    raw = project(2)
    gated = raw[:, :dk] * raw[:, dk:]
    gext[pl.ds(8, rows)] = gated
    halo_send[...] = gated[rows - 8 :]

    landed(yrecv.at[pl.ds(0, ny - 1)], st_recv.at[0])
    landed(ydec.at[pl.ds(0, ny - 1), line], st_recv.at[4])
    so_far = jnp.zeros((vrows, dk), F32)
    logs = jnp.zeros((1, dk), F32)
    for j in range(ny):
        pref[j] = so_far
        dec[pl.ds(j, 1)] = logs
        step = ydec[j, line]
        so_far = so_far * jnp.exp(step) + yrecv[j].astype(F32)
        logs = logs + step
    zbuf[z] = so_far.astype(BF16)
    zdec[z] = jnp.broadcast_to(logs, (8, dk))
    for d in far_first:
        for k, ref in ((1, zbuf.at[z]), (5, zdec.at[z, line])):
            remote(ref, ref, st_send.at[k], st_recv.at[k], {Z: lax.rem(z + d, nz)}).start()
    ship(halo_send, gext.at[pl.ds(0, 8)], st_send.at[3], st_recv.at[3], after)
    pass_on(3, 3, 4, 5)
    pass_on(4, 3, 4)

    landed(zbuf.at[pl.ds(0, nz - 1)], st_recv.at[1])
    landed(zdec.at[pl.ds(0, nz - 1), line], st_recv.at[5])
    carry = startt[y]
    for j in range(nz):
        later = carry * jnp.exp(zdec[j, line]) + zbuf[j].astype(F32)
        carry = jnp.where(j < z, later, carry)
    for j in range(ny):
        back_send[j] = (carry * jnp.exp(dec[pl.ds(j, 1)]) + pref[j]).astype(BF16)
    back_recv[y] = back_send[y]
    for d in far_first:
        to = lax.rem(y + d, ny)
        remote(back_send.at[to], back_recv.at[y], st_send.at[2], st_recv.at[2], {Y: to}).start()

    pass_on(4, 5)
    landed(gext.at[pl.ds(0, 8)], st_recv.at[3])
    first = jnp.logical_and(z == 0, y == 0)
    halo = jnp.where(first, 0.0, gext[pl.ds(0, 8)])
    gext[pl.ds(0, 8)] = halo
    conv = (
        taps_v[pl.ds(0, 1)] * gext[pl.ds(6, rows)]
        + taps_v[pl.ds(1, 1)] * gext[pl.ds(7, rows)]
        + taps_v[pl.ds(2, 1)] * gext[pl.ds(8, rows)]
    )
    done(3)
    raw = project(3)
    queries = silu(raw[:, :dk])
    gate_out = silu(raw[:, dk:])
    local, lifted = [], []
    for b in range(blocks):
        at = pl.ds(b * BLOCK, BLOCK)
        running = r_ref[at]
        mid = running[BLOCK // 2 - 1 : BLOCK // 2]
        q = queries[b * BLOCK : (b + 1) * BLOCK]
        scores = dot(
            q * jnp.exp(running - mid), w_ref[at] * jnp.exp(mid - running), ((1,), (1,)), HIGHEST
        )
        scores = jnp.where(causal, scores, 0.0)
        here = dot(scores, u_ref[at], ((1,), (0,)), HIGHEST)
        here = here + dot(q * jnp.exp(running), lprev[b], ((1,), (1,)), HIGHEST)
        local.append(here)
        lifted.append(q * jnp.exp(running + off_ref[pl.ds(b, 1)]))
    local = jnp.concatenate(local, axis=0)
    lifted = jnp.concatenate(lifted, axis=0)

    done(4)
    short = (project(4) * conv).astype(BF16)
    both[:, :, :, pl.ds(dk, dk)] = short.reshape(nx, nc, per, dk)
    landed(back_recv.at[pl.ds(0, ny - 1)], st_recv.at[2])
    carried = back_recv[...].reshape(dk, dk).astype(F32)
    mixed = local + dot(lifted, carried, ((1,), (1,)), HIGHEST)
    norm = lax.rsqrt(jnp.mean(mixed * mixed, axis=-1, keepdims=True) + EPS)
    rec = (mixed * norm * sgain_v[...] * gate_out).astype(BF16)
    both[:, :, :, pl.ds(0, dk)] = rec.reshape(nx, nc, per, dk)

    done(5)

    weights = whole(5)
    width = out.shape[1]
    chunks = 8
    size = width // chunks
    theirs = both[:, 1 - c].reshape(nx * per, 2 * dk)
    mine = both[:, c].reshape(nx * per, 2 * dk)

    def pair_ship(q):
        at = pl.ds(q * size, size)
        remote(psend.at[:, :, at], precv.at[:, :, at], pd_send, pd_recv.at[q], {C: 1 - c}).start()

    for q in range(chunks):
        part = dot(theirs, weights[q * size : (q + 1) * size], ((1,), (1,)))
        psend[:, :, pl.ds(q * size, size)] = part.astype(BF16).reshape(nx, per, size)
        if q > 0:
            pair_ship(q - 1)
    own = [dot(mine, weights[:size], ((1,), (1,)))]
    pair_ship(chunks - 1)

    part = size // 2
    ways = ((0, lax.rem(x + 1, nx)), (1, lax.rem(x + nx - 1, nx)))
    opposite = lax.rem(x + nx // 2, nx)
    relays = nx == 4

    def hop(src, dst, q, kind, d, to):
        remote(src, dst, px_send, px_recv.at[q, kind, d], {X: to}).start()

    def cols(q, d):
        return pl.ds(q * size + d * part, part)

    def push_far(q):
        if relays:
            for d, to in ways:
                hop(ssum.at[opposite, :, cols(q, d)], xrelay.at[:, cols(q, d)], q, 0, d, to)

    def push(q):
        for d, to in ways:
            hop(ssum.at[to, :, cols(q, 1 - d)], xrecv.at[d, :, cols(q, 1 - d)], q, 1, d, to)

    def push_added(q, way):
        d, to = way
        hop(ssum.at[to, :, cols(q, d)], xrecv.at[d, :, cols(q, d)], q, 2, d, to)

    for q in range(chunks):
        at = pl.ds(q * size, size)
        landed(precv.at[:, :, at], pd_recv.at[q])
        mix = own[q].reshape(nx, per, size) + precv[:, :, at].astype(F32)
        ssum[:, :, at] = mix.astype(BF16)
        if q < chunks - 1:
            own.append(dot(mine, weights[(q + 1) * size : (q + 2) * size], ((1,), (1,))))
        push_far(q)
    for q in range(chunks):
        push(q)
    if relays:
        held = None
        for q in range(chunks):
            for way in ways:
                d, to = way
                landed(xrelay.at[:, cols(q, d)], px_recv.at[q, 0, d])
                added = ssum[to, :, cols(q, d)].astype(F32) + xrelay[:, cols(q, d)].astype(F32)
                ssum[to, :, cols(q, d)] = added.astype(BF16)
                if held is not None:
                    push_added(*held)
                held = (q, way)
        push_added(*held)
    for q in range(chunks):
        at = pl.ds(q * size, size)
        acc = ssum[x, :, at].astype(F32)
        for d, to in ways:
            landed(xrecv.at[d, :, cols(q, 1 - d)], px_recv.at[q, 1, d])
            if relays:
                landed(xrecv.at[d, :, cols(q, d)], px_recv.at[q, 2, d])
        if relays:
            acc = acc + xrecv[0, :, at].astype(F32) + xrecv[1, :, at].astype(F32)
        else:
            ways_back = [xrecv[1 - h, :, cols(q, h)].astype(F32) for h in range(2)]
            acc = acc + jnp.concatenate(ways_back, axis=1)
        out[:, at] = acc.astype(BF16)

    for g in range(6):
        left(groups[g].at[pl.ds(0, n - 1), 0], p1_send.at[g])
        left(groups[g].at[pl.ds(0, n - 1)], r_send.at[g])
    left(ysend.at[pl.ds(0, ny - 1)], st_send.at[0])
    left(ydec.at[pl.ds(0, ny - 1), line], st_send.at[4])
    left(zbuf.at[pl.ds(0, nz - 1)], st_send.at[1])
    left(zdec.at[pl.ds(0, nz - 1), line], st_send.at[5])
    left(back_send.at[pl.ds(0, ny - 1)], st_send.at[2])
    left(psend, pd_send)
    left(ssum.at[pl.ds(0, nx - 1)], px_send)
    for copy in pending:
        copy.wait_send()


def on_device(sizes, *args):
    (
        tokens,
        norm_gain,
        w_query,
        w_forget,
        w_input,
        w_outgate,
        w_bgate,
        w_cgate,
        w_value,
        floor_gap,
        extra_decay,
        start_state,
        state_gain,
        conv_taps,
        out_rec,
        out_conv,
    ) = args
    nz, ny, nx, nc = sizes
    per, model = tokens.shape
    rows = per * nx * nc
    blocks = rows // BLOCK
    dk = floor_gap.shape[1]
    half = per // 2
    vrows = dk // ny
    vmem = pl.BlockSpec(memory_space=pltpu.VMEM)
    hbm = pl.BlockSpec(memory_space=pl.ANY)
    dma = pltpu.SemaphoreType.DMA
    steps = nz // 2
    gathered = [(nz, ny, 2, half, k * dk) for k in (1, 1, 2, 2, 1, 2)]
    operands = (
        tokens,
        norm_gain[None],
        w_query,
        w_forget,
        w_input,
        w_outgate,
        w_bgate,
        w_cgate,
        w_value,
        floor_gap,
        extra_decay.T,
        start_state,
        state_gain[None],
        conv_taps,
        out_rec.T,
        out_conv.T,
    )
    small = (1, 9, 10, 11, 12, 13)
    scratch = [
        pltpu.VMEM((nx, nc, per, model), BF16),
        *[pltpu.VMEM(shape, BF16) for shape in gathered],
        pltpu.VMEM((rows, model), BF16),
        pltpu.VMEM((blocks, dk), F32),
        pltpu.VMEM((rows, dk), F32),
        pltpu.VMEM((rows, dk), F32),
        pltpu.VMEM((rows, dk), F32),
        pltpu.VMEM((blocks, dk, dk), F32),
        pltpu.VMEM((ny, vrows, dk), F32),
        pltpu.VMEM((ny, vrows, dk), BF16),
        pltpu.VMEM((ny, vrows, dk), BF16),
        pltpu.VMEM((ny, 8, dk), F32),
        pltpu.VMEM((nz, vrows, dk), BF16),
        pltpu.VMEM((nz, 8, dk), F32),
        pltpu.VMEM((ny, vrows, dk), F32),
        pltpu.VMEM((ny, dk), F32),
        pltpu.VMEM((ny, vrows, dk), BF16),
        pltpu.VMEM((ny, vrows, dk), BF16),
        pltpu.VMEM((8, dk), F32),
        pltpu.VMEM((rows + 8, dk), F32),
        pltpu.VMEM((nx, nc, per, 2 * dk), BF16),
        *[pltpu.VMEM((nx, per, model), BF16)] * 3,
        pltpu.VMEM((per, model), BF16),
        pltpu.VMEM((2, per, model), BF16),
        *[pltpu.VMEM(operands[i].shape, F32) for i in small],
        dma((13,)),
        dma((6,)),
        dma((6,)),
        dma((steps, 2)),
        dma((6,)),
        dma((6, steps)),
        dma((2, nx // 2)),
        dma((2, nx // 2)),
        dma((nx,)),
        dma((nx,)),
        dma((6,)),
        dma((6,)),
        dma,
        dma((8,)),
        dma,
        dma((8, 3, 2)),
    ]
    return pl.pallas_call(
        functools.partial(kernel, sizes),
        out_shape=jax.ShapeDtypeStruct((per, model), BF16),
        in_specs=[hbm] * len(operands),
        out_specs=vmem,
        scratch_shapes=scratch,
        compiler_params=pltpu.CompilerParams(collective_id=0, has_side_effects=True),
    )(*operands)


def on_torus(devices, sizes):
    torus = Mesh(devices.reshape(sizes), SP_TP)
    return jax.shard_map(
        functools.partial(on_device, sizes),
        mesh=torus,
        in_specs=(
            P(SP_TP, None),
            P(),
            P(SP, TP),
            P(SP, TP),
            P(SP, TP),
            P(SP, TP),
            P(SP, TP),
            P(SP, TP),
            P(SP, TP),
            P(TP, None),
            P(SP, TP),
            P(TP, None, None),
            P(),
            P(None, TP),
            P(TP, SP),
            P(TP, SP),
        ),
        out_specs=P(SP_TP, None),
        check_vma=False,
    )


def solution(mesh):
    return on_torus(mesh.devices, (8, 8, 4, 2))
```
